256 devices in a mesh: ep: 128 (over z, y, x), tp: 2 (over core).
Axes of the slice: x: 4, y: 4, z: 8, core: 2. Of those that a mesh axis runs over, the one named last changes fastest.
Arguments:
- tokens: bfloat16 [4096, 2048], P('ep'), may hold values from -6 to 6
- lru_state: float32 [4096, 1024], P('ep', 'tp'), may hold values from -6 to 6
- conv_window: bfloat16 [4096, 3, 1024], P('ep', None, 'tp'), may hold values from -6 to 6
- gain_mix_in: float32 [2048], replicated, may hold values from 0.1 to 1.9
- gain_mix_out: float32 [2048], replicated, may hold values from 0.1 to 1.9
- gain_ffn_in: float32 [2048], replicated, may hold values from 0.1 to 1.9
- gain_ffn_out: float32 [2048], replicated, may hold values from 0.1 to 1.9
- w_branch: bfloat16 [2048, 1024], P(None, 'tp'), may hold values from -0.125 to 0.125
- w_input: bfloat16 [2048, 1024], P(None, 'tp'), may hold values from -0.125 to 0.125
- conv_taps: bfloat16 [4, 1024], P(None, 'tp'), may hold values from -3 to 3
- gate_a: bfloat16 [8, 128, 128], P('tp'), may hold values from -0.5 to 0.5
- gate_x: bfloat16 [8, 128, 128], P('tp'), may hold values from -0.5 to 0.5
- decay_rate: float32 [1024], P('tp'), may hold values from 0.001 to 0.3
- w_mix_out: bfloat16 [1024, 2048], P('tp'), may hold values from -0.1875 to 0.1875
- routes: int32 [4096, 4], P('ep'), may hold values from 0 to 127, all different within a row; in each aligned block of 32 rows (0 to 31, 32 to 63, ...) at most 2 rows name the same one
- route_weight: float32 [4096, 4], P('ep'), may hold values from 0.2 to 1.5
- expert_gate: bfloat16 [128, 2048, 512], P('ep', None, 'tp'), may hold values from -0.125 to 0.125
- expert_up: bfloat16 [128, 2048, 512], P('ep', None, 'tp'), may hold values from -0.125 to 0.125
- expert_down: bfloat16 [128, 512, 2048], P('ep', 'tp'), may hold values from -0.25 to 0.25
- shared_gate: bfloat16 [2048, 512], P(None, 'tp'), may hold values from -0.125 to 0.125
- shared_up: bfloat16 [2048, 512], P(None, 'tp'), may hold values from -0.125 to 0.125
- shared_down: bfloat16 [512, 2048], P('tp'), may hold values from -0.25 to 0.25
Outputs:
- layer_out: bfloat16 [4096, 2048], P('ep')
- new_state: float32 [4096, 1024], P('ep', 'tp')
- new_window: bfloat16 [4096, 3, 1024], P('ep', None, 'tp')
The draws below stay inside these ranges and needn't reach their ends.
Inputs may be any that keep to these rules, and one draw needn't show every extreme that they name: `routes`: each row names 4 different experts. Within the rows of one device (aligned blocks of 32 rows) no expert is named by more than 2 entries, a bound that some block reaches.
All inputs are finite; a program needn't handle non-finite values.
Results may differ from the reference program's by a relative error of at most 0.014.
Values may be sent and summed in bfloat16 or wider, within the bound.
A program may use at most 64 MiB of HBM per device.

```python
import math
import jax
import jax.numpy as jnp
import numpy as np
from jax import lax

D = 2048
DL = 1024
LRU_BLOCKS = 8
BD = 128
CONV_W = 4
FE = 512
SH = 512
TOP_K = 4
EXP_DEV = 1
EXPERTS = 128
SEQ_DEV = 32
TOKENS = 4096
CAP = 2
N_EP = 128
N_TP = 2


def shard_levels(own_key, extent, pieces, smallest, largest):
    def one(position, parts):
        heights = jax.random.uniform(jax.random.fold_in(jax.random.fold_in(own_key, 6), position), (parts,), jnp.float32, smallest / len(pieces), largest / len(pieces))
        return jnp.repeat(jnp.exp(heights), extent[position] // parts).reshape((-1,) + (1,) * (len(extent) - position - 1))

    level = one(*pieces[0])
    for cut in pieces[1:]:
        level = level * one(*cut)
    return level


def assign_block(key, own, number, rows, count, top, most, lean):
    sequence = jax.random.permutation(key, count)
    heavy_load, usual = portions_of(count, rows * top, most, lean, True), portions_of(count, rows * top, most, lean, False)
    places = jnp.arange(count)

    def named(tallies, turn):
        used = int((tallies > 0).sum())
        fixed = max(1, used // 4)
        passed = fixed + (places - fixed + turn * (used - fixed)) % max(1, count - fixed)
        return jnp.zeros((count,), jnp.int32).at[sequence[jnp.where(places < fixed, places, passed)]].set(jnp.asarray(tallies, jnp.int32))

    tallies = jnp.where(number % 4 == 0, named(heavy_load, number // 4), named(usual, number - number // 4 - 1))
    mixed = jax.random.permutation(jax.random.fold_in(own, 3), count)
    giver, receiver = mixed[0:count // 2 * 2:2], mixed[1:count // 2 * 2:2]
    room = jnp.minimum(tallies[giver] - 1, most - tallies[receiver]) // 2
    room = jnp.where((giver == sequence[0]) | (receiver == sequence[0]) | (tallies[receiver] == 0), 0, jnp.maximum(room, 0))
    passed = jax.random.randint(jax.random.fold_in(own, 4), (count // 2,), 0, 1 << 20) % (room + 1)
    tallies = tallies.at[giver].add(-passed).at[receiver].add(passed)
    items = jnp.searchsorted(jnp.cumsum(tallies), jnp.arange(rows * top), side="right").astype(jnp.int32)
    table = items.reshape(top, rows).T
    table = table[jax.random.permutation(jax.random.fold_in(own, 1), rows)]
    turn = jax.random.randint(jax.random.fold_in(own, 2), (rows, 1), 0, top)
    return jnp.take_along_axis(table, (jnp.arange(top)[None, :] + turn) % top, axis=1)


def portions_of(number_of, total, bound, skew, full):
    portions = [(1 << 20) // math.isqrt(rank ** skew) + 1 for rank in range(1, number_of + 1)]
    largest = bound if full else min(bound, max(-(-total // number_of), total * portions[0] // sum(portions)))
    least = 1 if total - largest >= number_of - 1 else 0
    holding, spare = [largest] + [least] * (number_of - 1), total - largest - least * (number_of - 1)
    while spare > 0:
        free = [i for i in range(1, number_of) if holding[i] < largest] or [i for i in range(1, number_of) if holding[i] < bound]
        pool, remaining = sum([portions[i] for i in free]), spare
        for i in free:
            more = min(bound - holding[i], max(1, remaining * portions[i] // pool), spare)
            holding[i] = holding[i] + more
            spare = spare - more
    return np.array(holding)


def scatter_about(stream_key, shape, scale, most, shards=(), kind=jnp.bfloat16):
    values = jax.random.normal(stream_key, shape, jnp.float32) * scale
    if len(shards) > 0:
        values = shard_levels(stream_key, shape, shards, -0.22, 0.18) * values
    return jnp.clip(values, min=-most, max=most).astype(kind)


def setup_inputs(seed: int = 0) -> dict:
    streams_of = jax.random.split(jax.random.key(seed), 23)
    tokens = scatter_about(streams_of[0], (TOKENS, D), 1.0, 6.0, ((0, 128),))
    lru_state = scatter_about(streams_of[1], (TOKENS, DL), 1.0, 6.0, ((0, 128), (1, 2)), jnp.float32)
    conv_window = scatter_about(streams_of[2], (TOKENS, CONV_W - 1, DL), 1.0, 6.0, ((0, 128), (2, 2)))
    gain_mix_in = jnp.clip(1.0 + 0.18 * jax.random.normal(streams_of[3], (D,), jnp.float32), 0.1, 1.9)
    gain_mix_out = jnp.clip(1.0 + 0.18 * jax.random.normal(streams_of[4], (D,), jnp.float32), 0.1, 1.9)
    gain_ffn_in = jnp.clip(1.0 + 0.18 * jax.random.normal(streams_of[5], (D,), jnp.float32), 0.1, 1.9)
    gain_ffn_out = jnp.clip(1.0 + 0.18 * jax.random.normal(streams_of[6], (D,), jnp.float32), 0.1, 1.9)
    w_branch = scatter_about(streams_of[7], (D, DL), D ** -0.5, 0.125, ((1, 2),))
    w_input = scatter_about(streams_of[8], (D, DL), D ** -0.5, 0.125, ((1, 2),))
    conv_taps = scatter_about(streams_of[9], (CONV_W, DL), 0.5, 3.0, ((1, 2),))
    gate_a = scatter_about(streams_of[10], (LRU_BLOCKS, BD, BD), BD ** -0.5, 0.5, ((0, 2),))
    gate_x = scatter_about(streams_of[11], (LRU_BLOCKS, BD, BD), BD ** -0.5, 0.5, ((0, 2),))
    decay_rate = jnp.clip(jnp.exp(math.log(0.3) - 5.7037825 * jax.random.uniform(streams_of[12], (DL,), jnp.float32) ** shard_levels(streams_of[12], (DL,), ((0, 2),), -0.2, 0.2)), 0.001, 0.3)
    w_mix_out = scatter_about(streams_of[13], (DL, D), DL ** -0.5, 0.1875, ((0, 2),))
    routes_keys = jax.random.split(jax.random.fold_in(streams_of[14], 1), TOKENS // SEQ_DEV)
    routes_turns = jax.random.permutation(jax.random.fold_in(streams_of[14], 3), TOKENS // SEQ_DEV)
    routes = jax.vmap(lambda own, number: assign_block(jax.random.fold_in(streams_of[14], 2), own, number, SEQ_DEV, EXP_DEV * N_EP, TOP_K, CAP, 2))(routes_keys, routes_turns).reshape((TOKENS, TOP_K))
    route_weight = jnp.clip(jnp.exp(math.log(1.5) - 2.014903 * jax.random.uniform(streams_of[15], (TOKENS, TOP_K), jnp.float32) ** shard_levels(streams_of[15], (TOKENS, TOP_K), ((0, 128),), -0.2, 0.2)), 0.2, 1.5)
    expert_gate = scatter_about(streams_of[16], (EXPERTS, D, FE), D ** -0.5, 0.125, ((0, 128), (2, 2)))
    expert_up = scatter_about(streams_of[17], (EXPERTS, D, FE), D ** -0.5, 0.125, ((0, 128), (2, 2)))
    expert_down = scatter_about(streams_of[18], (EXPERTS, FE, D), FE ** -0.5, 0.25, ((0, 128), (1, 2)))
    shared_gate = scatter_about(streams_of[19], (D, SH), D ** -0.5, 0.125, ((1, 2),))
    shared_up = scatter_about(streams_of[20], (D, SH), D ** -0.5, 0.125, ((1, 2),))
    shared_down = scatter_about(streams_of[21], (SH, D), SH ** -0.5, 0.25, ((0, 2),))
    return dict(tokens=tokens, lru_state=lru_state, conv_window=conv_window, gain_mix_in=gain_mix_in, gain_mix_out=gain_mix_out, gain_ffn_in=gain_ffn_in, gain_ffn_out=gain_ffn_out, w_branch=w_branch, w_input=w_input, conv_taps=conv_taps, gate_a=gate_a, gate_x=gate_x, decay_rate=decay_rate, w_mix_out=w_mix_out, routes=routes, route_weight=route_weight, expert_gate=expert_gate, expert_up=expert_up, expert_down=expert_down, shared_gate=shared_gate, shared_up=shared_up, shared_down=shared_down)


def rms_norm(value, gain):
    return value * lax.rsqrt(lax.optimization_barrier(jnp.mean(value * value, axis=-1, keepdims=True)) + 1e-06) * gain

def parted(hidden, weight):
    width = hidden.shape[1]
    step = width // N_TP
    total = jnp.zeros((hidden.shape[0], weight.shape[1]), jnp.float32)
    for part in range(N_TP):
        piece = jnp.dot(hidden[:, part * step:(part + 1) * step], weight[part * step:(part + 1) * step], preferred_element_type=jnp.float32).astype(jnp.bfloat16)
        piece = lax.optimization_barrier(piece)
        total = total + piece.astype(jnp.float32)
    return total

def reference(tokens, lru_state, conv_window, gain_mix_in, gain_mix_out, gain_ffn_in, gain_ffn_out, w_branch, w_input, conv_taps, gate_a, gate_x, decay_rate, w_mix_out, routes, route_weight, expert_gate, expert_up, expert_down, shared_gate, shared_up, shared_down):
    resid = tokens.astype(jnp.float32)
    normed = rms_norm(resid, gain_mix_in).astype(jnp.bfloat16)
    branch = jnp.dot(normed, w_branch, preferred_element_type=jnp.float32)
    inflow = jnp.dot(normed, w_input, preferred_element_type=jnp.float32).astype(jnp.bfloat16)
    window = jnp.concatenate([conv_window, inflow[:, None, :]], axis=1)
    new_window = window[:, 1:]
    conv = lax.optimization_barrier(jnp.sum(window.astype(jnp.float32) * conv_taps.astype(jnp.float32)[None], axis=1))
    count = conv.shape[0]
    grouped = conv.astype(jnp.bfloat16).astype(jnp.float32).reshape(count, LRU_BLOCKS, BD)
    recur_gate = jax.nn.sigmoid(jnp.einsum('sbi,bij->sbj', grouped, gate_a.astype(jnp.float32)).reshape(count, DL))
    input_gate = jax.nn.sigmoid(jnp.einsum('sbi,bij->sbj', grouped, gate_x.astype(jnp.float32)).reshape(count, DL))
    log_decay = -8.0 * recur_gate * decay_rate[None]
    new_state = jnp.exp(log_decay) * lru_state + jnp.sqrt(-jnp.expm1(2.0 * log_decay)) * conv * input_gate
    gated = (new_state * jax.nn.gelu(branch)).astype(jnp.bfloat16)
    mixed = parted(gated, w_mix_out)
    middle = (resid + rms_norm(mixed, gain_mix_out)).astype(jnp.bfloat16)
    ffn_in = rms_norm(middle.astype(jnp.float32), gain_ffn_in).astype(jnp.bfloat16)
    shared_hidden = (jax.nn.silu(jnp.dot(ffn_in, shared_gate, preferred_element_type=jnp.float32)) * jnp.dot(ffn_in, shared_up, preferred_element_type=jnp.float32)).astype(jnp.bfloat16)
    shared = parted(shared_hidden, shared_down)
    per_block = SEQ_DEV * TOP_K
    flat = routes.reshape(N_EP, per_block)
    onehot = (flat[:, :, None] == jnp.arange(EXPERTS, dtype=jnp.int32)[None, None, :]).astype(jnp.int32)
    rank = lax.optimization_barrier(jnp.sum(onehot * (jnp.cumsum(onehot, axis=1) - 1), axis=-1))
    places = N_EP * CAP
    block_id = jnp.arange(N_EP, dtype=jnp.int32)[:, None]
    dest = (flat * places + block_id * CAP + rank).astype(jnp.int32)
    source = (block_id * SEQ_DEV + jnp.arange(per_block, dtype=jnp.int32)[None, :] // TOP_K).astype(jnp.int32)
    table = jnp.full((EXPERTS * places,), TOKENS, jnp.int32).at[dest.reshape(-1)].set(source.reshape(-1))
    table = table.reshape(EXPERTS, places)
    padded = jnp.concatenate([ffn_in, jnp.zeros((1, D), jnp.bfloat16)], axis=0)

    def one_expert(item):
        index, weight_g, weight_u, weight_d = item
        rows = padded[index]
        hidden = (jax.nn.silu(jnp.dot(rows, weight_g, preferred_element_type=jnp.float32)) * jnp.dot(rows, weight_u, preferred_element_type=jnp.float32)).astype(jnp.bfloat16)
        return parted(hidden, weight_d).astype(jnp.bfloat16)
    expert_out = lax.map(one_expert, (table, expert_gate, expert_up, expert_down))
    picked = expert_out.reshape(EXPERTS * places, D)[dest.reshape(-1)].reshape(TOKENS, TOP_K, D)
    routed = lax.optimization_barrier(jnp.sum(picked.astype(jnp.float32) * route_weight[:, :, None], axis=1)).astype(jnp.bfloat16)
    total = routed.astype(jnp.float32) + shared
    layer_out = (middle.astype(jnp.float32) + rms_norm(total, gain_ffn_out)).astype(jnp.bfloat16)
    return (layer_out, new_state, new_window)
```

```python
import functools

import jax
import jax.numpy as jnp
from jax import lax
from jax.experimental import pallas as pl
from jax.experimental.pallas import tpu as pltpu
from jax.sharding import PartitionSpec as P

MESH = pl.DeviceIdType.MESH
F32 = jnp.float32
BF16 = jnp.bfloat16

NZ = 8
NQ = 16
SEQ = 32
TOP = 4
D = 2048
HALF = D // 2
NCH = 2
CW = HALF // NCH
LC = 512
HID = 256
ROWS = NZ * 2
NPIECE = 4


def scaled(value, gain):
    return value * lax.rsqrt(jnp.mean(value * value, axis=-1, keepdims=True) + 1e-06) * gain


def dot(a, b):
    return jnp.dot(a, b, preferred_element_type=F32)


def kernel(
    tok_h, lru_h, convp_h, taps_h, gains_h, decay_h, wb_h, wi_h, ga_h, gx_h, wm_h, routes_h, meta_h,
    eg_h, eu_h, ed_h, sg_h, su_h, sd_h,
    out_h, state_h, inflow_h,
    tok, lru, convp, taps, gains, decay, wb, wi, ga, gx, wm, routes, meta_in,
    eg, eu, ed, sg, su, sd,
    state_v, inflow_v, out_v, middle_v, ffn,
    mix_s, mix_r, meta_s, meta_r, sh_s, sh_r,
    g_buf, r_buf, x_buf, p_buf, whi, wlo, hid_v, y_s, y_r, o_buf, b_buf, t_buf, v_buf, rt_buf,
    lsem, osem,
    tp_s, tp_r, ms_s, ms_r, za_s, za_r, xa_s, xa_r, xf_s, xf_r, yx_s, yx_r, xb_s, xb_r, zb_s, zb_r, rt_s, rt_r,
):
    me = lax.axis_index("ep")
    c = lax.axis_index("tp")
    z = me // NQ
    q = me % NQ
    y, x = q // 4, q % 4

    def z_peer(i):
        return lax.rem(z + i, NZ)

    def q_peer(i):
        return lax.rem(y + i // 4, 4) * 4 + lax.rem(x + i % 4, 4)

    def rows(i, n):
        return pl.ds(pl.multiple_of(i * n, n), n)

    barrier = pltpu.get_barrier_semaphore()
    pl.semaphore_signal(barrier, inc=1, device_id=(me, 1 - c), device_id_type=MESH)

    def greet_z(i, carry):
        pl.semaphore_signal(barrier, inc=1, device_id=(z_peer(i) * NQ + q, c), device_id_type=MESH)
        return carry

    def greet_q(i, carry):
        pl.semaphore_signal(barrier, inc=1, device_id=(z * NQ + q_peer(i), c), device_id_type=MESH)
        return carry

    lax.fori_loop(1, NZ, greet_z, 0)
    lax.fori_loop(1, NQ, greet_q, 0)

    def load(k, src, dst):
        copy = pltpu.make_async_copy(src, dst, lsem.at[k])
        copy.start()
        return copy

    step = D // NPIECE
    l_tok = load(0, tok_h, tok)
    l_gains = load(1, gains_h, gains)
    l_wi = [load(2 + i, wi_h.at[pl.ds(i * step, step)], wi.at[pl.ds(i * step, step)]) for i in range(NPIECE)]
    l_convp = load(6, convp_h, convp)
    l_taps = load(7, taps_h, taps)
    l_ga = load(8, ga_h, ga)
    l_gx = load(9, gx_h, gx)
    l_wb = [load(10 + i, wb_h.at[pl.ds(i * step, step)], wb.at[pl.ds(i * step, step)]) for i in range(NPIECE)]
    l_decay = load(14, decay_h, decay)
    l_lru = load(15, lru_h, lru)
    l_routes = load(16, routes_h, routes)
    l_meta = load(17, meta_h, meta_in)
    l_wm = load(18, wm_h, wm)

    l_routes.wait()
    l_meta.wait()
    lane = lax.broadcasted_iota(jnp.int32, (1, NZ * SEQ), 1)
    mine = (lane // SEQ) == z
    earlier = lax.broadcasted_iota(jnp.int32, (SEQ, NZ * SEQ), 0) < (lane % SEQ)
    named = routes[...].astype(F32)
    for k in range(TOP):
        expert = meta_in[k : k + 1, :]
        same = named[:, 0:1] == expert
        for j in range(1, TOP):
            same = same | (named[:, j : j + 1] == expert)
        rank = jnp.sum(jnp.where(same & earlier, 1.0, 0.0), axis=0, keepdims=True)
        meta_s[k : k + 1, :] = jnp.where(mine, 2.0 * expert + rank, 0.0)
    meta_s[TOP : 2 * TOP, :] = jnp.where(mine, meta_in[TOP : 2 * TOP, :], 0.0)
    meta_r[pl.ds(z, 1)] = meta_s[...][None]

    l_tok.wait()
    l_gains.wait()
    normed = scaled(tok[...].astype(F32), gains[0:1, :]).astype(BF16)
    inflow = jnp.zeros((SEQ, LC), F32)
    for i in range(NPIECE):
        l_wi[i].wait()
        inflow += dot(normed[:, i * step : (i + 1) * step], wi[i * step : (i + 1) * step, :])
    inflow = inflow.astype(BF16)
    inflow_v[...] = inflow
    o_inflow = pltpu.make_async_copy(inflow_v, inflow_h, osem.at[0])
    o_inflow.start()
    l_convp.wait()
    l_taps.wait()
    conv = convp[...] + inflow.astype(F32) * taps[3:4, :].astype(F32)
    low = conv.astype(BF16)
    l_ga.wait()
    l_gx.wait()
    groups = LC // 128
    recur = [dot(low[:, g * 128 : (g + 1) * 128], ga[g]) for g in range(groups)]
    inputs = [dot(low[:, g * 128 : (g + 1) * 128], gx[g]) for g in range(groups)]
    recur_gate = jax.nn.sigmoid(jnp.concatenate(recur, axis=1))
    input_gate = jax.nn.sigmoid(jnp.concatenate(inputs, axis=1))
    l_decay.wait()
    l_lru.wait()
    fall = 8.0 * recur_gate * decay[...]
    t = jnp.tanh(fall)
    state = jnp.exp(-fall) * lru[...] + jnp.sqrt(2.0 * t / (1.0 + t)) * conv * input_gate
    state_v[...] = state
    o_state = pltpu.make_async_copy(state_v, state_h, osem.at[1])
    o_state.start()
    branch = jnp.zeros((SEQ, LC), F32)
    for i in range(NPIECE):
        l_wb[i].wait()
        branch += dot(normed[:, i * step : (i + 1) * step], wb[i * step : (i + 1) * step, :])
    gated = (state * jax.nn.gelu(branch)).astype(BF16)
    l_wm.wait()
    mix_s[...] = dot(gated, wm[...]).astype(BF16)

    l_sg = load(19, sg_h, sg)
    l_su = load(20, su_h, su)
    l_sd = load(21, sd_h, sd)
    l_eg = load(22, eg_h, eg)
    l_eu = load(23, eu_h, eu)
    l_ed = [load(24 + i, ed_h.at[:, pl.ds(i * HALF, HALF)], ed.at[i]) for i in range(2)]

    pl.semaphore_wait(barrier, 1 + (NZ - 1) + (NQ - 1))

    def remote(src, dst, ssem, rsem, e, t):
        return pltpu.make_async_remote_copy(
            src_ref=src, dst_ref=dst, send_sem=ssem, recv_sem=rsem, device_id=(e, t), device_id_type=MESH
        )

    mix_copy = remote(mix_s, mix_r, tp_s.at[0], tp_r.at[0], me, 1 - c)
    mix_copy.start()

    def meta_copy(i, to):
        return remote(meta_s, meta_r.at[to], ms_s.at[i], ms_r.at[to], z_peer(i) * NQ + q, c)

    def meta_send(i, carry):
        meta_copy(i, z).start()
        return carry

    lax.fori_loop(1, NZ, meta_send, 0)

    mix_copy.wait()
    mixed = mix_s[...].astype(F32) + mix_r[...].astype(F32)
    middle = (tok[...].astype(F32) + scaled(mixed, gains[1:2, :])).astype(BF16)
    middle_v[...] = middle
    ffn[...] = scaled(middle.astype(F32), gains[2:3, :]).astype(BF16)

    def z_out(ch, i):
        block = rows(z, SEQ)
        return remote(
            g_buf.at[ch, block], g_buf.at[ch, block], za_s.at[ch, i], za_r.at[ch, z], z_peer(i) * NQ + q, c
        )

    def z_in(ch, i):
        block = rows(z_peer(i), SEQ)
        return remote(
            g_buf.at[ch, block], g_buf.at[ch, block], za_s.at[ch, i], za_r.at[ch, z_peer(i)], z_peer(i) * NQ + q, c
        )

    for ch in range(NCH):
        g_buf[ch, rows(z, SEQ), :] = ffn[:, pl.ds(pl.multiple_of(c * HALF + ch * CW, CW), CW)]

        def z_send(i, carry, ch=ch):
            z_out(ch, i).start()
            return carry

        lax.fori_loop(1, NZ, z_send, 0)

    l_sg.wait()
    l_su.wait()
    l_sd.wait()
    hidden = (jax.nn.silu(dot(ffn[...], sg[...])) * dot(ffn[...], su[...])).astype(BF16)
    sh_s[...] = dot(hidden, sd[...]).astype(BF16)
    sh_copy = remote(sh_s, sh_r, tp_s.at[1], tp_r.at[1], me, 1 - c)
    sh_copy.start()

    def meta_wait(i, carry):
        meta_copy(i, z_peer(i)).wait()
        return carry

    lax.fori_loop(1, NZ, meta_wait, 0)
    meta = jnp.sum(meta_r[...], axis=0)
    code = meta[0:TOP, :].astype(jnp.int32)
    place = ((code % (2 * NQ)) // 2) * ROWS + (lane // SEQ) * 2 + code % 2
    place = jnp.where(code // (2 * NQ) == z, place, -1)
    row = lax.broadcasted_iota(jnp.int32, (NQ * ROWS, NZ * SEQ), 0)
    filled = jnp.zeros((NQ * ROWS, NZ * SEQ), F32)
    weight = jnp.zeros((NQ * ROWS, NZ * SEQ), F32)
    for k in range(TOP):
        hit = row == place[k : k + 1, :]
        filled = jnp.where(hit, 1.0, filled)
        weight = jnp.where(hit, meta[TOP + k : TOP + k + 1, :], weight)
    p_buf[...] = filled.astype(BF16)
    weight = weight.T
    high = weight.astype(BF16)
    whi[...] = high
    wlo[...] = (weight - high.astype(F32)).astype(BF16)

    def q_copy(src, dst, ss, rs, ch, i, at):
        p = q_peer(i)
        return remote(src.at[ch, rows(p, ROWS)], dst.at[rows(at, ROWS)], ss.at[ch, i], rs.at[ch, at], z * NQ + p, c)

    for ch in range(NCH):

        def z_wait(i, carry, ch=ch):
            z_in(ch, i).wait()
            return carry

        lax.fori_loop(1, NZ, z_wait, 0)
        r_buf[ch] = dot(p_buf[...], g_buf[ch]).astype(BF16)

        def q_send(i, carry, ch=ch):
            q_copy(r_buf, x_buf.at[c, ch], xa_s, xa_r, ch, i, q).start()
            return carry

        lax.fori_loop(1, NQ, q_send, 0)
        x_buf[c, ch, rows(q, ROWS), :] = r_buf[ch, rows(q, ROWS), :]

    l_eg.wait()
    l_eu.wait()
    gate = jnp.zeros((NQ * ROWS, HID), F32)
    up = jnp.zeros((NQ * ROWS, HID), F32)
    forwards = []
    for ch in range(NCH):

        def q_wait(i, carry, ch=ch):
            q_copy(r_buf, x_buf.at[c, ch], xa_s, xa_r, ch, i, q_peer(i)).wait()
            return carry

        lax.fori_loop(1, NQ, q_wait, 0)
        copy = remote(x_buf.at[c, ch], x_buf.at[c, ch], xf_s.at[ch], xf_r.at[ch], me, 1 - c)
        copy.start()
        forwards.append(copy)
        depth = rows(c * NCH + ch, CW)
        gate += dot(x_buf[c, ch], eg[0, depth, :])
        up += dot(x_buf[c, ch], eu[0, depth, :])
    for ch in range(NCH):
        other = remote(x_buf.at[1 - c, ch], x_buf.at[1 - c, ch], xf_s.at[ch], xf_r.at[ch], me, 1 - c)
        other.wait_recv()
        forwards[ch].wait_send()
        depth = rows((1 - c) * NCH + ch, CW)
        gate += dot(x_buf[1 - c, ch], eg[0, depth, :])
        up += dot(x_buf[1 - c, ch], eu[0, depth, :])
    hid_v[...] = (jax.nn.silu(gate) * up).astype(BF16)

    for copy in l_ed:
        copy.wait()
    trades = []
    for ch in range(NCH):
        y_s[ch] = dot(hid_v[...], ed[1 - c, :, ch * CW : (ch + 1) * CW]).astype(BF16)
        copy = remote(y_s.at[ch], y_r.at[ch], yx_s.at[ch], yx_r.at[ch], me, 1 - c)
        copy.start()
        trades.append(copy)
    for ch in range(NCH):
        own = dot(hid_v[...], ed[c, :, ch * CW : (ch + 1) * CW]).astype(BF16).astype(F32)
        trades[ch].wait()
        o_buf[ch] = (own + y_r[ch].astype(F32)).astype(BF16)

        def back_send(i, carry, ch=ch):
            q_copy(o_buf, b_buf.at[ch], xb_s, xb_r, ch, i, q).start()
            return carry

        lax.fori_loop(1, NQ, back_send, 0)
        b_buf[ch, rows(q, ROWS), :] = o_buf[ch, rows(q, ROWS), :]

    def sum_copy(ch, i, at):
        p = z_peer(i)
        return remote(
            t_buf.at[ch, rows(p, SEQ)], v_buf.at[ch, rows(at, SEQ)], zb_s.at[ch, i], zb_r.at[ch, at], p * NQ + q, c
        )

    for ch in range(NCH):

        def back_wait(i, carry, ch=ch):
            q_copy(o_buf, b_buf.at[ch], xb_s, xb_r, ch, i, q_peer(i)).wait()
            return carry

        lax.fori_loop(1, NQ, back_wait, 0)
        t_buf[ch] = (dot(whi[...], b_buf[ch]) + dot(wlo[...], b_buf[ch])).astype(BF16)

        def sum_send(i, carry, ch=ch):
            sum_copy(ch, i, z).start()
            return carry

        lax.fori_loop(1, NZ, sum_send, 0)
        v_buf[ch, rows(z, SEQ), :] = t_buf[ch, rows(z, SEQ), :]

    sh_copy.wait()
    shared = sh_s[...].astype(F32) + sh_r[...].astype(F32)
    pairs = []
    for ch in range(NCH):

        def sum_wait(i, carry, ch=ch):
            sum_copy(ch, i, z_peer(i)).wait()
            return carry

        lax.fori_loop(1, NZ, sum_wait, 0)
        total = v_buf[ch, 0:SEQ, :].astype(F32)
        for s in range(1, NZ):
            total += v_buf[ch, s * SEQ : (s + 1) * SEQ, :].astype(F32)
        rt_buf[c, ch] = total.astype(BF16)
        copy = remote(rt_buf.at[c, ch], rt_buf.at[c, ch], rt_s.at[ch], rt_r.at[ch], me, 1 - c)
        copy.start()
        pairs.append(copy)
    for ch in range(NCH):
        remote(rt_buf.at[1 - c, ch], rt_buf.at[1 - c, ch], rt_s.at[ch], rt_r.at[ch], me, 1 - c).wait_recv()
        pairs[ch].wait_send()
    routed = jnp.concatenate([rt_buf[h, ch] for h in range(2) for ch in range(NCH)], axis=1)
    last = scaled(routed.astype(F32) + shared, gains[3:4, :])
    out_v[...] = (middle_v[...].astype(F32) + last).astype(BF16)
    o_out = pltpu.make_async_copy(out_v, out_h, osem.at[2])
    o_out.start()
    o_inflow.wait()
    o_state.wait()
    o_out.wait()


def on_device(
    tokens, lru_state, conv_window, gain_mix_in, gain_mix_out, gain_ffn_in, gain_ffn_out, w_branch, w_input,
    conv_taps, gate_a, gate_x, decay_rate, w_mix_out, routes, route_weight, expert_gate, expert_up, expert_down,
    shared_gate, shared_up, shared_down,
):
    taps = conv_taps.astype(F32)
    convp = jnp.sum(conv_window.astype(F32) * taps[None, :3], axis=1)
    gains = jnp.stack([gain_mix_in, gain_mix_out, gain_ffn_in, gain_ffn_out])
    meta = jnp.tile(jnp.concatenate([routes.astype(F32), route_weight], axis=1).T, (1, NZ))
    hbm = pl.BlockSpec(memory_space=pltpu.HBM)

    def vmem(*shape, dtype=BF16):
        return pltpu.VMEM(shape, dtype)

    def dma(*shape):
        return pltpu.SemaphoreType.DMA(shape)

    scratch = [
        vmem(SEQ, D), vmem(SEQ, LC, dtype=F32), vmem(SEQ, LC, dtype=F32), vmem(4, LC), vmem(4, D, dtype=F32),
        vmem(1, LC, dtype=F32), vmem(D, LC), vmem(D, LC), vmem(4, 128, 128), vmem(4, 128, 128), vmem(LC, D),
        vmem(SEQ, TOP, dtype=jnp.int32), vmem(2 * TOP, NZ * SEQ, dtype=F32),
        vmem(1, D, HID), vmem(1, D, HID), vmem(2, HID, HALF), vmem(D, HID), vmem(D, HID), vmem(HID, D),
        vmem(SEQ, LC, dtype=F32), vmem(SEQ, LC), vmem(SEQ, D), vmem(SEQ, D), vmem(SEQ, D),
        vmem(SEQ, D), vmem(SEQ, D), vmem(2 * TOP, NZ * SEQ, dtype=F32), vmem(NZ, 2 * TOP, NZ * SEQ, dtype=F32),
        vmem(SEQ, D), vmem(SEQ, D),
        vmem(NCH, NZ * SEQ, CW), vmem(NCH, NQ * ROWS, CW), vmem(2, NCH, NQ * ROWS, CW),
        vmem(NQ * ROWS, NZ * SEQ), vmem(NZ * SEQ, NQ * ROWS), vmem(NZ * SEQ, NQ * ROWS), vmem(NQ * ROWS, HID),
        vmem(NCH, NQ * ROWS, CW), vmem(NCH, NQ * ROWS, CW), vmem(NCH, NQ * ROWS, CW), vmem(NCH, NQ * ROWS, CW),
        vmem(NCH, NZ * SEQ, CW), vmem(NCH, NZ * SEQ, CW), vmem(2, NCH, SEQ, CW),
        dma(26), dma(3),
        dma(2), dma(2), dma(NZ), dma(NZ), dma(NCH, NZ), dma(NCH, NZ), dma(NCH, NQ), dma(NCH, NQ), dma(NCH), dma(NCH),
        dma(NCH), dma(NCH), dma(NCH, NQ), dma(NCH, NQ), dma(NCH, NZ), dma(NCH, NZ), dma(NCH), dma(NCH),
    ]
    layer_out, new_state, inflow = pl.pallas_call(
        kernel,
        out_shape=(
            jax.ShapeDtypeStruct((SEQ, D), BF16),
            jax.ShapeDtypeStruct((SEQ, LC), F32),
            jax.ShapeDtypeStruct((SEQ, LC), BF16),
        ),
        in_specs=[hbm] * 19,
        out_specs=(hbm,) * 3,
        scratch_shapes=scratch,
        compiler_params=pltpu.CompilerParams(collective_id=0, has_side_effects=True, vmem_limit_bytes=60 * 2**20),
        name="layer",
    )(
        tokens, lru_state, convp, conv_taps, gains, decay_rate[None], w_branch, w_input, gate_a, gate_x, w_mix_out,
        routes, meta, expert_gate, expert_up, expert_down[0], shared_gate, shared_up, shared_down,
    )
    new_window = jnp.concatenate([conv_window[:, 1:], inflow[:, None, :]], axis=1)
    return (layer_out, new_state, new_window)


def solution(mesh):
    placed = (
        P("ep", None),
        P("ep", "tp"),
        P("ep", None, "tp"),
        P(),
        P(),
        P(),
        P(),
        P(None, "tp"),
        P(None, "tp"),
        P(None, "tp"),
        P("tp", None, None),
        P("tp", None, None),
        P("tp"),
        P("tp", None),
        P("ep", None),
        P("ep", None),
        P("ep", None, "tp"),
        P("ep", None, "tp"),
        P("ep", "tp", None),
        P(None, "tp"),
        P(None, "tp"),
        P("tp", None),
    )
    return jax.shard_map(
        on_device,
        mesh=mesh,
        in_specs=placed,
        out_specs=(P("ep", None), P("ep", "tp"), P("ep", None, "tp")),
        check_vma=False,
    )
```

```python
import functools

import jax
import jax.numpy as jnp
from jax import lax
from jax.experimental import pallas as pl
from jax.experimental.pallas import tpu as pltpu
from jax.sharding import PartitionSpec as P

MESH = pl.DeviceIdType.MESH
F32 = jnp.float32
BF16 = jnp.bfloat16

NZ = 8
NQ = 16
SEQ = 32
TOP = 4
D = 2048
HALF = D // 2
NCH = 2
CW = HALF // NCH
LC = 512
HID = 256
ROWS = NZ * 2
NPIECE = 4


def scaled(value, gain):
    return value * lax.rsqrt(jnp.mean(value * value, axis=-1, keepdims=True) + 1e-06) * gain


def dot(a, b):
    return jnp.dot(a, b, preferred_element_type=F32)


def kernel(
    tok_h, lru_h, win_h, taps_h, gain0_h, gain1_h, gain2_h, gain3_h, decay_h, wb_h, wi_h, ga_h, gx_h, wm_h,
    routes_h, rweight_h, eg_h, eu_h, ed_h, sg_h, su_h, sd_h,
    out_v, state_v, window_v,
    tok, lru, win, taps, gains, decay, wb, wi, ga, gx, wm, routes, rweight,
    eg, eu, ed, sg, su, sd,
    middle_v, ffn,
    mix_s, mix_r, meta_s, meta_r, sh_s, sh_r,
    g_buf, r_buf, x_buf, p_buf, whi, wlo, hid_v, y_s, y_r, o_buf, b_buf, t_buf, v_buf, rt_buf,
    lsem,
    tp_s, tp_r, ms_s, ms_r, za_s, za_r, xa_s, xa_r, xf_s, xf_r, yx_s, yx_r, xb_s, xb_r, zb_s, zb_r, rt_s, rt_r,
):
    me = lax.axis_index("ep")
    c = lax.axis_index("tp")
    z = me // NQ
    q = me % NQ
    y, x = q // 4, q % 4

    def z_peer(i):
        return lax.rem(z + i, NZ)

    def q_peer(i):
        return lax.rem(y + i // 4, 4) * 4 + lax.rem(x + i % 4, 4)

    def rows(i, n):
        return pl.ds(pl.multiple_of(i * n, n), n)

    barrier = pltpu.get_barrier_semaphore()
    pl.semaphore_signal(barrier, inc=1, device_id=(me, 1 - c), device_id_type=MESH)

    def greet_z(i, carry):
        pl.semaphore_signal(barrier, inc=1, device_id=(z_peer(i) * NQ + q, c), device_id_type=MESH)
        return carry

    def greet_q(i, carry):
        pl.semaphore_signal(barrier, inc=1, device_id=(z * NQ + q_peer(i), c), device_id_type=MESH)
        return carry

    lax.fori_loop(1, NZ, greet_z, 0)
    lax.fori_loop(1, NQ, greet_q, 0)

    def load(k, src, dst):
        copy = pltpu.make_async_copy(src, dst, lsem.at[k])
        copy.start()
        return copy

    step = D // NPIECE
    l_tok = load(0, tok_h, tok)
    l_gains = [load(1 + i, h, gains.at[i]) for i, h in enumerate((gain0_h, gain1_h, gain2_h, gain3_h))]
    l_wi = [load(5 + i, wi_h.at[pl.ds(i * step, step)], wi.at[pl.ds(i * step, step)]) for i in range(NPIECE)]
    l_win = load(9, win_h, win)
    l_taps = load(10, taps_h, taps)
    l_ga = load(11, ga_h, ga)
    l_gx = load(12, gx_h, gx)
    l_routes = load(13, routes_h, routes)
    l_rweight = load(14, rweight_h, rweight)
    l_wb = [load(15 + i, wb_h.at[pl.ds(i * step, step)], wb.at[pl.ds(i * step, step)]) for i in range(NPIECE)]
    l_decay = load(19, decay_h, decay)
    l_lru = load(20, lru_h, lru)
    l_wm = load(21, wm_h, wm)

    with jax.named_scope("slots"):
        l_routes.wait()
        l_rweight.wait()
        lane = lax.broadcasted_iota(jnp.int32, (1, NZ * SEQ), 1)
        mine = (lane // SEQ) == z
        earlier = lax.broadcasted_iota(jnp.int32, (SEQ, NZ * SEQ), 0) < (lane % SEQ)
        diagonal = lax.broadcasted_iota(jnp.int32, (SEQ, SEQ), 0) == lax.broadcasted_iota(jnp.int32, (SEQ, SEQ), 1)
        narrow = routes[...].astype(F32)
        named = [
            jnp.sum(jnp.where(diagonal, narrow[k : k + 1, :], 0.0), axis=1, keepdims=True) for k in range(TOP)
        ]
        wide = jnp.concatenate([narrow] * NZ, axis=1)
        for k in range(TOP):
            expert = wide[k : k + 1, :]
            same = named[0] == expert
            for j in range(1, TOP):
                same = same | (named[j] == expert)
            rank = jnp.sum(jnp.where(same & earlier, 1.0, 0.0), axis=0, keepdims=True)
            meta_s[k : k + 1, :] = jnp.where(mine, 2.0 * expert + rank, 0.0)
        meta_s[TOP : 2 * TOP, :] = jnp.where(mine, jnp.concatenate([rweight[...]] * NZ, axis=1), 0.0)
        meta_r[pl.ds(z, 1)] = meta_s[...][None]

    l_tok.wait()
    for copy in l_gains:
        copy.wait()
    normed = scaled(tok[...].astype(F32), gains[0]).astype(BF16)
    inflow = jnp.zeros((SEQ, LC), F32)
    for i in range(NPIECE):
        l_wi[i].wait()
        inflow += dot(normed[:, i * step : (i + 1) * step], wi[i * step : (i + 1) * step, :])
    inflow = inflow.astype(BF16)
    l_win.wait()
    l_taps.wait()
    conv = inflow.astype(F32) * taps[3:4, :].astype(F32)
    for j in range(3):
        conv += win[j].astype(F32) * taps[j : j + 1, :].astype(F32)
        window_v[j] = win[j + 1] if j < 2 else inflow
    low = conv.astype(BF16)
    l_ga.wait()
    l_gx.wait()
    groups = LC // 128
    recur = [dot(low[:, g * 128 : (g + 1) * 128], ga[g]) for g in range(groups)]
    inputs = [dot(low[:, g * 128 : (g + 1) * 128], gx[g]) for g in range(groups)]
    recur_gate = jax.nn.sigmoid(jnp.concatenate(recur, axis=1))
    input_gate = jax.nn.sigmoid(jnp.concatenate(inputs, axis=1))
    l_decay.wait()
    l_lru.wait()
    fall = 8.0 * recur_gate * decay[...]
    t = jnp.tanh(fall)
    state = jnp.exp(-fall) * lru[...] + jnp.sqrt(2.0 * t / (1.0 + t)) * conv * input_gate
    state_v[...] = state
    branch = jnp.zeros((SEQ, LC), F32)
    for i in range(NPIECE):
        l_wb[i].wait()
        branch += dot(normed[:, i * step : (i + 1) * step], wb[i * step : (i + 1) * step, :])
    gated = (state * jax.nn.gelu(branch)).astype(BF16)
    l_wm.wait()
    mix_s[...] = dot(gated, wm[...]).astype(BF16)

    l_sg = load(22, sg_h, sg)
    l_su = load(23, su_h, su)
    l_sd = load(24, sd_h, sd)
    l_eg = load(25, eg_h, eg)
    l_eu = load(26, eu_h, eu)
    l_ed = [load(27 + i, ed_h.at[:, pl.ds(i * HALF, HALF)], ed.at[i]) for i in range(2)]

    pl.semaphore_wait(barrier, 1 + (NZ - 1) + (NQ - 1))

    def remote(src, dst, ssem, rsem, e, t):
        return pltpu.make_async_remote_copy(
            src_ref=src, dst_ref=dst, send_sem=ssem, recv_sem=rsem, device_id=(e, t), device_id_type=MESH
        )

    mix_copy = remote(mix_s, mix_r, tp_s.at[0], tp_r.at[0], me, 1 - c)
    mix_copy.start()

    def meta_copy(i, to):
        return remote(meta_s, meta_r.at[to], ms_s.at[i], ms_r.at[to], z_peer(i) * NQ + q, c)

    def meta_send(i, carry):
        meta_copy(i, z).start()
        return carry

    lax.fori_loop(1, NZ, meta_send, 0)

    mix_copy.wait()
    mixed = mix_s[...].astype(F32) + mix_r[...].astype(F32)
    middle = (tok[...].astype(F32) + scaled(mixed, gains[1])).astype(BF16)
    middle_v[...] = middle
    ffn[...] = scaled(middle.astype(F32), gains[2]).astype(BF16)

    def z_out(ch, i):
        block = rows(z, SEQ)
        return remote(
            g_buf.at[ch, block], g_buf.at[ch, block], za_s.at[ch, i], za_r.at[ch, z], z_peer(i) * NQ + q, c
        )

    def z_in(ch, i):
        block = rows(z_peer(i), SEQ)
        return remote(
            g_buf.at[ch, block], g_buf.at[ch, block], za_s.at[ch, i], za_r.at[ch, z_peer(i)], z_peer(i) * NQ + q, c
        )

    for ch in range(NCH):
        g_buf[ch, rows(z, SEQ), :] = ffn[:, pl.ds(pl.multiple_of(c * HALF + ch * CW, CW), CW)]

        def z_send(i, carry, ch=ch):
            z_out(ch, i).start()
            return carry

        lax.fori_loop(1, NZ, z_send, 0)

    l_sg.wait()
    l_su.wait()
    l_sd.wait()
    hidden = (jax.nn.silu(dot(ffn[...], sg[...])) * dot(ffn[...], su[...])).astype(BF16)
    sh_s[...] = dot(hidden, sd[...]).astype(BF16)
    sh_copy = remote(sh_s, sh_r, tp_s.at[1], tp_r.at[1], me, 1 - c)
    sh_copy.start()

    def meta_wait(i, carry):
        meta_copy(i, z_peer(i)).wait()
        return carry

    lax.fori_loop(1, NZ, meta_wait, 0)
    meta = jnp.sum(meta_r[...], axis=0)
    code = meta[0:TOP, :].astype(jnp.int32)
    place = ((code % (2 * NQ)) // 2) * ROWS + (lane // SEQ) * 2 + code % 2
    place = jnp.where(code // (2 * NQ) == z, place, -1)
    row = lax.broadcasted_iota(jnp.int32, (NQ * ROWS, NZ * SEQ), 0)
    filled = jnp.zeros((NQ * ROWS, NZ * SEQ), F32)
    weight = jnp.zeros((NQ * ROWS, NZ * SEQ), F32)
    for k in range(TOP):
        hit = row == place[k : k + 1, :]
        filled = jnp.where(hit, 1.0, filled)
        weight = jnp.where(hit, meta[TOP + k : TOP + k + 1, :], weight)
    p_buf[...] = filled.astype(BF16)
    weight = weight.T
    high = weight.astype(BF16)
    whi[...] = high
    wlo[...] = (weight - high.astype(F32)).astype(BF16)

    def q_copy(src, dst, ss, rs, ch, i, at):
        p = q_peer(i)
        return remote(src.at[ch, rows(p, ROWS)], dst.at[rows(at, ROWS)], ss.at[ch, i], rs.at[ch, at], z * NQ + p, c)

    for ch in range(NCH):

        def z_wait(i, carry, ch=ch):
            z_in(ch, i).wait()
            return carry

        lax.fori_loop(1, NZ, z_wait, 0)
        r_buf[ch] = dot(p_buf[...], g_buf[ch]).astype(BF16)

        def q_send(i, carry, ch=ch):
            q_copy(r_buf, x_buf.at[c, ch], xa_s, xa_r, ch, i, q).start()
            return carry

        lax.fori_loop(1, NQ, q_send, 0)
        x_buf[c, ch, rows(q, ROWS), :] = r_buf[ch, rows(q, ROWS), :]

    l_eg.wait()
    l_eu.wait()
    gate = jnp.zeros((NQ * ROWS, HID), F32)
    up = jnp.zeros((NQ * ROWS, HID), F32)
    forwards = []
    for ch in range(NCH):

        def q_wait(i, carry, ch=ch):
            q_copy(r_buf, x_buf.at[c, ch], xa_s, xa_r, ch, i, q_peer(i)).wait()
            return carry

        lax.fori_loop(1, NQ, q_wait, 0)
        copy = remote(x_buf.at[c, ch], x_buf.at[c, ch], xf_s.at[ch], xf_r.at[ch], me, 1 - c)
        copy.start()
        forwards.append(copy)
        depth = rows(c * NCH + ch, CW)
        gate += dot(x_buf[c, ch], eg[0, depth, :])
        up += dot(x_buf[c, ch], eu[0, depth, :])
    for ch in range(NCH):
        other = remote(x_buf.at[1 - c, ch], x_buf.at[1 - c, ch], xf_s.at[ch], xf_r.at[ch], me, 1 - c)
        other.wait_recv()
        forwards[ch].wait_send()
        depth = rows((1 - c) * NCH + ch, CW)
        gate += dot(x_buf[1 - c, ch], eg[0, depth, :])
        up += dot(x_buf[1 - c, ch], eu[0, depth, :])
    hid_v[...] = (jax.nn.silu(gate) * up).astype(BF16)

    for copy in l_ed:
        copy.wait()
    trades = []
    for ch in range(NCH):
        y_s[ch] = dot(hid_v[...], ed[1 - c, :, ch * CW : (ch + 1) * CW]).astype(BF16)
        copy = remote(y_s.at[ch], y_r.at[ch], yx_s.at[ch], yx_r.at[ch], me, 1 - c)
        copy.start()
        trades.append(copy)
    for ch in range(NCH):
        own = dot(hid_v[...], ed[c, :, ch * CW : (ch + 1) * CW]).astype(BF16).astype(F32)
        trades[ch].wait()
        o_buf[ch] = (own + y_r[ch].astype(F32)).astype(BF16)

        def back_send(i, carry, ch=ch):
            q_copy(o_buf, b_buf.at[ch], xb_s, xb_r, ch, i, q).start()
            return carry

        lax.fori_loop(1, NQ, back_send, 0)
        b_buf[ch, rows(q, ROWS), :] = o_buf[ch, rows(q, ROWS), :]

    def sum_copy(ch, i, at):
        p = z_peer(i)
        return remote(
            t_buf.at[ch, rows(p, SEQ)], v_buf.at[ch, rows(at, SEQ)], zb_s.at[ch, i], zb_r.at[ch, at], p * NQ + q, c
        )

    for ch in range(NCH):

        def back_wait(i, carry, ch=ch):
            q_copy(o_buf, b_buf.at[ch], xb_s, xb_r, ch, i, q_peer(i)).wait()
            return carry

        lax.fori_loop(1, NQ, back_wait, 0)
        t_buf[ch] = (dot(whi[...], b_buf[ch]) + dot(wlo[...], b_buf[ch])).astype(BF16)

        def sum_send(i, carry, ch=ch):
            sum_copy(ch, i, z).start()
            return carry

        lax.fori_loop(1, NZ, sum_send, 0)
        v_buf[ch, rows(z, SEQ), :] = t_buf[ch, rows(z, SEQ), :]

    sh_copy.wait()
    shared = sh_s[...].astype(F32) + sh_r[...].astype(F32)
    pairs = []
    for ch in range(NCH):

        def sum_wait(i, carry, ch=ch):
            sum_copy(ch, i, z_peer(i)).wait()
            return carry

        lax.fori_loop(1, NZ, sum_wait, 0)
        total = v_buf[ch, 0:SEQ, :].astype(F32)
        for s in range(1, NZ):
            total += v_buf[ch, s * SEQ : (s + 1) * SEQ, :].astype(F32)
        rt_buf[c, ch] = total.astype(BF16)
        copy = remote(rt_buf.at[c, ch], rt_buf.at[c, ch], rt_s.at[ch], rt_r.at[ch], me, 1 - c)
        copy.start()
        pairs.append(copy)
    for ch in range(NCH):
        remote(rt_buf.at[1 - c, ch], rt_buf.at[1 - c, ch], rt_s.at[ch], rt_r.at[ch], me, 1 - c).wait_recv()
        pairs[ch].wait_send()
    routed = jnp.concatenate([rt_buf[h, ch] for h in range(2) for ch in range(NCH)], axis=1)
    last = scaled(routed.astype(F32) + shared, gains[3])
    out_v[...] = (middle_v[...].astype(F32) + last).astype(BF16)


def store(*refs):
    n = len(refs) // 2
    copies = [pltpu.make_async_copy(refs[i], refs[n + i], refs[-1].at[i]) for i in range(n)]
    for copy in copies:
        copy.start()
    for copy in copies:
        copy.wait()


def on_device(
    tokens, lru_state, conv_window, gain_mix_in, gain_mix_out, gain_ffn_in, gain_ffn_out, w_branch, w_input,
    conv_taps, gate_a, gate_x, decay_rate, w_mix_out, routes, route_weight, expert_gate, expert_up, expert_down,
    shared_gate, shared_up, shared_down,
):
    hbm = pl.BlockSpec(memory_space=pltpu.HBM)

    def vmem(*shape, dtype=BF16):
        return pltpu.VMEM(shape, dtype)

    def dma(*shape):
        return pltpu.SemaphoreType.DMA(shape)

    scratch = [
        vmem(SEQ, D), vmem(SEQ, LC, dtype=F32), vmem(3, SEQ, LC), vmem(4, LC), vmem(4, 1, D, dtype=F32),
        vmem(1, LC, dtype=F32), vmem(D, LC), vmem(D, LC), vmem(4, 128, 128), vmem(4, 128, 128), vmem(LC, D),
        vmem(TOP, SEQ, dtype=jnp.int32), vmem(TOP, SEQ, dtype=F32),
        vmem(1, D, HID), vmem(1, D, HID), vmem(2, HID, HALF), vmem(D, HID), vmem(D, HID), vmem(HID, D),
        vmem(SEQ, D), vmem(SEQ, D),
        vmem(SEQ, D), vmem(SEQ, D), vmem(2 * TOP, NZ * SEQ, dtype=F32), vmem(NZ, 2 * TOP, NZ * SEQ, dtype=F32),
        vmem(SEQ, D), vmem(SEQ, D),
        vmem(NCH, NZ * SEQ, CW), vmem(NCH, NQ * ROWS, CW), vmem(2, NCH, NQ * ROWS, CW),
        vmem(NQ * ROWS, NZ * SEQ), vmem(NZ * SEQ, NQ * ROWS), vmem(NZ * SEQ, NQ * ROWS), vmem(NQ * ROWS, HID),
        vmem(NCH, NQ * ROWS, CW), vmem(NCH, NQ * ROWS, CW), vmem(NCH, NQ * ROWS, CW), vmem(NCH, NQ * ROWS, CW),
        vmem(NCH, NZ * SEQ, CW), vmem(NCH, NZ * SEQ, CW), vmem(2, NCH, SEQ, CW),
        dma(29),
        dma(2), dma(2), dma(NZ), dma(NZ), dma(NCH, NZ), dma(NCH, NZ), dma(NCH, NQ), dma(NCH, NQ), dma(NCH), dma(NCH),
        dma(NCH), dma(NCH), dma(NCH, NQ), dma(NCH, NQ), dma(NCH, NZ), dma(NCH, NZ), dma(NCH), dma(NCH),
    ]
    vm = pl.BlockSpec(memory_space=pltpu.VMEM)
    results = pl.pallas_call(
        kernel,
        out_shape=(
            pltpu.VMEM((SEQ, D), BF16),
            pltpu.VMEM((SEQ, LC), F32),
            pltpu.VMEM((3, SEQ, LC), BF16),
        ),
        in_specs=[hbm] * 22,
        out_specs=(vm,) * 3,
        scratch_shapes=scratch,
        compiler_params=pltpu.CompilerParams(collective_id=0, has_side_effects=True, vmem_limit_bytes=60 * 2**20),
        name="layer",
    )(
        tokens, lru_state, conv_window.transpose(1, 0, 2), conv_taps, gain_mix_in[None], gain_mix_out[None],
        gain_ffn_in[None], gain_ffn_out[None], decay_rate[None], w_branch, w_input, gate_a, gate_x, w_mix_out,
        routes.T, route_weight.T, expert_gate, expert_up, expert_down[0], shared_gate, shared_up, shared_down,
    )
    layer_out, new_state, window = pl.pallas_call(
        store,
        out_shape=tuple(jax.ShapeDtypeStruct(r.shape, r.dtype) for r in results),
        in_specs=[vm] * 3,
        out_specs=(hbm,) * 3,
        scratch_shapes=[dma(3)],
        compiler_params=pltpu.CompilerParams(has_side_effects=True, vmem_limit_bytes=2**20),
        name="store",
    )(*results)
    return (layer_out, new_state, window.transpose(1, 0, 2))


def solution(mesh):
    placed = (
        P("ep", None),
        P("ep", "tp"),
        P("ep", None, "tp"),
        P(),
        P(),
        P(),
        P(),
        P(None, "tp"),
        P(None, "tp"),
        P(None, "tp"),
        P("tp", None, None),
        P("tp", None, None),
        P("tp"),
        P("tp", None),
        P("ep", None),
        P("ep", None),
        P("ep", None, "tp"),
        P("ep", None, "tp"),
        P("ep", "tp", None),
        P(None, "tp"),
        P(None, "tp"),
        P("tp", None),
    )
    return jax.shard_map(
        on_device,
        mesh=mesh,
        in_specs=placed,
        out_specs=(P("ep", None), P("ep", "tp"), P("ep", None, "tp")),
        check_vma=False,
    )
```

```python
import functools

import jax
import jax.numpy as jnp
from jax import lax
from jax.experimental import pallas as pl
from jax.experimental.pallas import tpu as pltpu
from jax.sharding import PartitionSpec as P

MESH = pl.DeviceIdType.MESH
F32 = jnp.float32
BF16 = jnp.bfloat16

NZ = 8
NQ = 16
SEQ = 32
TOP = 4
D = 2048
HALF = D // 2
NCH = 4
CW = HALF // NCH
LC = 512
HID = 256
ROWS = NZ * 2
NPIECE = 4


def scaled(value, gain):
    return value * lax.rsqrt(jnp.mean(value * value, axis=-1, keepdims=True) + 1e-06) * gain


def dot(a, b):
    return jnp.dot(a, b, preferred_element_type=F32)


def kernel(
    tok_h, lru_h, win_h, taps_h, gain0_h, gain1_h, gain2_h, gain3_h, decay_h, wb_h, wi_h, ga_h, gx_h, wm_h,
    routes_h, rweight_h, eg_h, eu_h, ed_h, sg_h, su_h, sd_h,
    out_v, state_v, window_v,
    tok, lru, win, taps, gains, decay, wb, wi, ga, gx, wm, routes, rweight,
    eg, eu, ed, sg, su, sd,
    middle_v, ffn,
    mix_s, mix_r, meta_s, meta_r, sh_s, sh_r,
    g_buf, r_buf, x_buf, p_buf, whi, wlo, hid_v, y_s, y_r, o_buf, b_buf, t_buf, rl_buf, c_buf, v_buf, rt_buf,
    lsem,
    tp_s, tp_r, ms_s, ms_r, za_s, za_two, za_r, xa_s, xa_r, xf_s, xf_r, yx_s, yx_r, xb_s, xb_r,
    zb_s, zb_two, zb_r, rt_s, rt_r,
):
    me = lax.axis_index("ep")
    c = lax.axis_index("tp")
    z = me // NQ
    q = me % NQ
    y, x = q // 4, q % 4

    def z_peer(i):
        return lax.rem(z + (i + NZ), NZ)

    def q_peer(i):
        return lax.rem(y + i // 4, 4) * 4 + lax.rem(x + i % 4, 4)

    def rows(i, n):
        return pl.ds(pl.multiple_of(i * n, n), n)

    barrier = pltpu.get_barrier_semaphore()
    pl.semaphore_signal(barrier, inc=1, device_id=(me, 1 - c), device_id_type=MESH)

    def greet_z(i, carry):
        pl.semaphore_signal(barrier, inc=1, device_id=(z_peer(i) * NQ + q, c), device_id_type=MESH)
        return carry

    def greet_q(i, carry):
        pl.semaphore_signal(barrier, inc=1, device_id=(z * NQ + q_peer(i), c), device_id_type=MESH)
        return carry

    lax.fori_loop(1, NZ, greet_z, 0)
    lax.fori_loop(1, NQ, greet_q, 0)

    def load(k, src, dst):
        copy = pltpu.make_async_copy(src, dst, lsem.at[k])
        copy.start()
        return copy

    step = D // NPIECE
    l_tok = load(0, tok_h, tok)
    l_gains = [load(1 + i, h, gains.at[i]) for i, h in enumerate((gain0_h, gain1_h, gain2_h, gain3_h))]
    l_wi = [load(5 + i, wi_h.at[pl.ds(i * step, step)], wi.at[pl.ds(i * step, step)]) for i in range(NPIECE)]
    l_win = load(9, win_h, win)
    l_taps = load(10, taps_h, taps)
    l_ga = load(11, ga_h, ga)
    l_gx = load(12, gx_h, gx)
    l_routes = load(13, routes_h, routes)
    l_rweight = load(14, rweight_h, rweight)
    l_wb = [load(15 + i, wb_h.at[pl.ds(i * step, step)], wb.at[pl.ds(i * step, step)]) for i in range(NPIECE)]
    l_decay = load(19, decay_h, decay)
    l_lru = load(20, lru_h, lru)
    l_wm = load(21, wm_h, wm)

    l_tok.wait()
    for copy in l_gains:
        copy.wait()
    normed = scaled(tok[...].astype(F32), gains[0]).astype(BF16)
    inflow = jnp.zeros((SEQ, LC), F32)
    for i in range(NPIECE):
        l_wi[i].wait()
        inflow += dot(normed[:, i * step : (i + 1) * step], wi[i * step : (i + 1) * step, :])
    inflow = inflow.astype(BF16)
    l_win.wait()
    l_taps.wait()
    conv = inflow.astype(F32) * taps[3:4, :].astype(F32)
    for j in range(3):
        conv += win[j].astype(F32) * taps[j : j + 1, :].astype(F32)
        window_v[j] = win[j + 1] if j < 2 else inflow
    low = conv.astype(BF16)
    l_ga.wait()
    l_gx.wait()
    groups = LC // 128
    recur = [dot(low[:, g * 128 : (g + 1) * 128], ga[g]) for g in range(groups)]
    inputs = [dot(low[:, g * 128 : (g + 1) * 128], gx[g]) for g in range(groups)]
    recur_gate = jax.nn.sigmoid(jnp.concatenate(recur, axis=1))
    input_gate = jax.nn.sigmoid(jnp.concatenate(inputs, axis=1))
    l_decay.wait()
    l_lru.wait()
    fall = 8.0 * recur_gate * decay[...]
    t = jnp.tanh(fall)
    state = jnp.exp(-fall) * lru[...] + jnp.sqrt(2.0 * t / (1.0 + t)) * conv * input_gate
    state_v[...] = state
    branch = jnp.zeros((SEQ, LC), F32)
    for i in range(NPIECE):
        l_wb[i].wait()
        branch += dot(normed[:, i * step : (i + 1) * step], wb[i * step : (i + 1) * step, :])
    gated = (state * jax.nn.gelu(branch)).astype(BF16)
    l_wm.wait()
    for i in range(2):
        mix_s[i] = dot(gated, wm[:, i * HALF : (i + 1) * HALF]).astype(BF16)

    l_sg = load(22, sg_h, sg)
    l_su = load(23, su_h, su)
    l_sd = load(24, sd_h, sd)
    l_eg = load(25, eg_h, eg)
    l_eu = load(26, eu_h, eu)
    l_ed = [load(27 + i, ed_h.at[:, pl.ds(i * HALF, HALF)], ed.at[i]) for i in range(2)]

    pl.semaphore_wait(barrier, 1 + (NZ - 1) + (NQ - 1))

    def remote(src, dst, ssem, rsem, e, t):
        return pltpu.make_async_remote_copy(
            src_ref=src, dst_ref=dst, send_sem=ssem, recv_sem=rsem, device_id=(e, t), device_id_type=MESH
        )

    def to_z(src, dst, ssem, rsem, i):
        return remote(src, dst, ssem, rsem, z_peer(i) * NQ + q, c)

    def to_core(src, dst, ssem, rsem):
        return remote(src, dst, ssem, rsem, me, 1 - c)

    mix_copies = [to_core(mix_s.at[i], mix_r.at[i], tp_s.at[i], tp_r.at[i]) for i in range(2)]
    for copy in mix_copies:
        copy.start()

    with jax.named_scope("slots"):
        l_routes.wait()
        l_rweight.wait()
        lane = lax.broadcasted_iota(jnp.int32, (1, NZ * SEQ), 1)
        mine = (lane // SEQ) == z
        earlier = lax.broadcasted_iota(jnp.int32, (SEQ, NZ * SEQ), 0) < (lane % SEQ)
        diagonal = lax.broadcasted_iota(jnp.int32, (SEQ, SEQ), 0) == lax.broadcasted_iota(jnp.int32, (SEQ, SEQ), 1)
        narrow = routes[...].astype(F32)
        named = [
            jnp.sum(jnp.where(diagonal, narrow[k : k + 1, :], 0.0), axis=1, keepdims=True) for k in range(TOP)
        ]
        wide = jnp.concatenate([narrow] * NZ, axis=1)
        for k in range(TOP):
            expert = wide[k : k + 1, :]
            same = named[0] == expert
            for j in range(1, TOP):
                same = same | (named[j] == expert)
            rank = jnp.sum(jnp.where(same & earlier, 1.0, 0.0), axis=0, keepdims=True)
            meta_s[k : k + 1, :] = jnp.where(mine, 2.0 * expert + rank, 0.0)
        meta_s[TOP : 2 * TOP, :] = jnp.where(mine, jnp.concatenate([rweight[...]] * NZ, axis=1), 0.0)
        meta_r[pl.ds(z, 1)] = meta_s[...][None]

    def meta_send(i, carry):
        to_z(meta_s, meta_r.at[z], ms_s, ms_r, i).start()
        return carry

    lax.fori_loop(1, NZ, meta_send, 0)

    mixed = []
    for i in range(2):
        mix_copies[i].wait()
        mixed.append(mix_s[i].astype(F32) + mix_r[i].astype(F32))
    mixed = jnp.concatenate(mixed, axis=1)
    middle = (tok[...].astype(F32) + scaled(mixed, gains[1])).astype(BF16)
    middle_v[...] = middle
    ffn[...] = scaled(middle.astype(F32), gains[2]).astype(BF16)

    def z_copy(ch, source, i, rsem):
        block = g_buf.at[ch, rows(source, SEQ)]
        return to_z(block, block, za_s.at[ch], rsem, i)

    for ch in range(NCH):
        g_buf[ch, rows(z, SEQ), :] = ffn[:, pl.ds(pl.multiple_of(c * HALF + ch * CW, CW), CW)]
        z_copy(ch, z, 2, za_two.at[ch, 0]).start()
        z_copy(ch, z, -2, za_two.at[ch, 1]).start()
        z_copy(ch, z, 1, za_r.at[ch]).start()
        z_copy(ch, z, -1, za_r.at[ch]).start()

    l_sg.wait()
    l_su.wait()
    l_sd.wait()
    hidden = (jax.nn.silu(dot(ffn[...], sg[...])) * dot(ffn[...], su[...])).astype(BF16)
    sh_s[...] = dot(hidden, sd[...]).astype(BF16)
    sh_copy = to_core(sh_s, sh_r, tp_s.at[2], tp_r.at[2])
    sh_copy.start()

    for ch in range(NCH):
        for way in range(2):
            sign = 1 - 2 * way
            source = z_peer(-2 * sign)
            z_copy(ch, source, sign, za_two.at[ch, way]).wait_recv()
            z_copy(ch, source, sign, za_r.at[ch]).start()
            if ch % 2 == way:
                z_copy(ch, source, 2 * sign, za_r.at[ch]).start()

    many = meta_r.at[pl.ds(0, NZ - 1)]
    to_z(many, many, ms_s, ms_r, 1).wait()
    meta = jnp.sum(meta_r[...], axis=0)
    code = meta[0:TOP, :].astype(jnp.int32)
    place = ((code % (2 * NQ)) // 2) * ROWS + (lane // SEQ) * 2 + code % 2
    place = jnp.where(code // (2 * NQ) == z, place, -1)
    row = lax.broadcasted_iota(jnp.int32, (NQ * ROWS, NZ * SEQ), 0)
    filled = jnp.zeros((NQ * ROWS, NZ * SEQ), F32)
    weight = jnp.zeros((NQ * ROWS, NZ * SEQ), F32)
    for k in range(TOP):
        hit = row == place[k : k + 1, :]
        filled = jnp.where(hit, 1.0, filled)
        weight = jnp.where(hit, meta[TOP + k : TOP + k + 1, :], weight)
    p_buf[...] = filled.astype(BF16)
    weight = weight.T
    high = weight.astype(BF16)
    whi[...] = high
    wlo[...] = (weight - high.astype(F32)).astype(BF16)

    def q_send(src, dst, ssem, rsem):
        def send(i, carry):
            p = q_peer(i)
            remote(src.at[rows(p, ROWS)], dst.at[rows(q, ROWS)], ssem, rsem, z * NQ + p, c).start()
            return carry

        lax.fori_loop(1, NQ, send, 0)

    def q_all(buf, ssem, rsem):
        part = buf.at[pl.ds(0, (NQ - 1) * ROWS)]
        return remote(part, part, ssem, rsem, z * NQ + q_peer(1), c)

    for ch in range(NCH):
        part = g_buf.at[ch, pl.ds(0, 5 * SEQ)]
        to_z(part, part, za_s.at[ch], za_r.at[ch], 1).wait_recv()
        r_buf[ch] = dot(p_buf[...], g_buf[ch]).astype(BF16)
        q_send(r_buf.at[ch], x_buf.at[c, ch], xa_s.at[ch], xa_r.at[ch])
        x_buf[c, ch, rows(q, ROWS), :] = r_buf[ch, rows(q, ROWS), :]

    l_eg.wait()
    l_eu.wait()
    gate = jnp.zeros((NQ * ROWS, HID), F32)
    up = jnp.zeros((NQ * ROWS, HID), F32)
    forwards = []
    for ch in range(NCH):
        q_all(x_buf.at[c, ch], xa_s.at[ch], xa_r.at[ch]).wait_recv()
        copy = to_core(x_buf.at[c, ch], x_buf.at[c, ch], xf_s.at[ch], xf_r.at[ch])
        copy.start()
        forwards.append(copy)
        depth = rows(c * NCH + ch, CW)
        gate += dot(x_buf[c, ch], eg[0, depth, :])
        up += dot(x_buf[c, ch], eu[0, depth, :])
    for ch in range(NCH):
        other = to_core(x_buf.at[1 - c, ch], x_buf.at[1 - c, ch], xf_s.at[ch], xf_r.at[ch])
        other.wait_recv()
        depth = rows((1 - c) * NCH + ch, CW)
        gate += dot(x_buf[1 - c, ch], eg[0, depth, :])
        up += dot(x_buf[1 - c, ch], eu[0, depth, :])
    hid_v[...] = (jax.nn.silu(gate) * up).astype(BF16)

    for copy in l_ed:
        copy.wait()
    trades = []
    for ch in range(NCH):
        y_s[ch] = dot(hid_v[...], ed[1 - c, :, ch * CW : (ch + 1) * CW]).astype(BF16)
        copy = to_core(y_s.at[ch], y_r.at[ch], yx_s.at[ch], yx_r.at[ch])
        copy.start()
        trades.append(copy)
    for ch in range(NCH):
        own = dot(hid_v[...], ed[c, :, ch * CW : (ch + 1) * CW]).astype(BF16).astype(F32)
        trades[ch].wait()
        o_buf[ch] = (own + y_r[ch].astype(F32)).astype(BF16)
        q_send(o_buf.at[ch], b_buf.at[ch], xb_s.at[ch], xb_r.at[ch])
        b_buf[ch, rows(q, ROWS), :] = o_buf[ch, rows(q, ROWS), :]

    def weighted(ch):
        q_all(b_buf.at[ch], xb_s.at[ch], xb_r.at[ch]).wait_recv()
        t_buf[ch] = (dot(whi[...], b_buf[ch]) + dot(wlo[...], b_buf[ch])).astype(BF16)
        for way in range(2):
            sign = 1 - 2 * way
            two = zb_two.at[ch, way]
            if ch % 2 == way:
                to_z(t_buf.at[ch, rows(z_peer(4), SEQ)], rl_buf.at[ch, way, 1], zb_s.at[ch], two, -2 * sign).start()
            to_z(t_buf.at[ch, rows(z_peer(-3 * sign), SEQ)], rl_buf.at[ch, way, 0], zb_s.at[ch], two, -sign).start()
        for way in range(2):
            sign = 1 - 2 * way
            to_z(t_buf.at[ch, rows(z_peer(-sign), SEQ)], v_buf.at[ch, way], zb_s.at[ch], zb_r.at[ch], -sign).start()

    def relayed(ch):
        for way in range(2):
            sign = 1 - 2 * way
            many = rl_buf.at[ch, way, pl.ds(0, 2 if ch % 2 == way else 1)]
            to_z(many, many, zb_s.at[ch], zb_two.at[ch, way], 1).wait_recv()
            total = t_buf[ch, rows(z_peer(-2 * sign), SEQ), :].astype(F32) + rl_buf[ch, way, 0].astype(F32)
            if ch % 2 == way:
                total += rl_buf[ch, way, 1].astype(F32)
            c_buf[ch, way] = total.astype(BF16)
            to_z(c_buf.at[ch, way], v_buf.at[ch, 2 + way], zb_s.at[ch], zb_r.at[ch], -2 * sign).start()

    for ch in range(NCH):
        weighted(ch)
        if ch >= 2:
            relayed(ch - 2)
    for ch in range(NCH - 2, NCH):
        relayed(ch)

    sh_copy.wait()
    shared = sh_s[...].astype(F32) + sh_r[...].astype(F32)
    pairs = []
    for ch in range(NCH):
        to_z(v_buf.at[ch], v_buf.at[ch], zb_s.at[ch], zb_r.at[ch], 1).wait_recv()
        total = t_buf[ch, rows(z, SEQ), :].astype(F32)
        for s in range(4):
            total += v_buf[ch, s].astype(F32)
        rt_buf[c, ch] = total.astype(BF16)
        copy = to_core(rt_buf.at[c, ch], rt_buf.at[c, ch], rt_s.at[ch], rt_r.at[ch])
        copy.start()
        pairs.append(copy)
    for ch in range(NCH):
        to_core(rt_buf.at[1 - c, ch], rt_buf.at[1 - c, ch], rt_s.at[ch], rt_r.at[ch]).wait_recv()
    routed = jnp.concatenate([rt_buf[h, ch] for h in range(2) for ch in range(NCH)], axis=1)
    last = scaled(routed.astype(F32) + shared, gains[3])
    out_v[...] = (middle_v[...].astype(F32) + last).astype(BF16)

    for ch in range(NCH):
        for buf, sem in ((g_buf, za_s), (t_buf, zb_s)):
            part = buf.at[ch, pl.ds(0, 7 * SEQ)]
            to_z(part, part, sem.at[ch], za_r.at[ch], 1).wait_send()
        q_all(r_buf.at[ch], xa_s.at[ch], xa_r.at[ch]).wait_send()
        q_all(o_buf.at[ch], xb_s.at[ch], xb_r.at[ch]).wait_send()
        forwards[ch].wait_send()
        pairs[ch].wait_send()


def store(*refs):
    n = len(refs) // 2
    copies = [pltpu.make_async_copy(refs[i], refs[n + i], refs[-1].at[i]) for i in range(n)]
    for copy in copies:
        copy.start()
    for copy in copies:
        copy.wait()


def on_device(
    tokens, lru_state, conv_window, gain_mix_in, gain_mix_out, gain_ffn_in, gain_ffn_out, w_branch, w_input,
    conv_taps, gate_a, gate_x, decay_rate, w_mix_out, routes, route_weight, expert_gate, expert_up, expert_down,
    shared_gate, shared_up, shared_down,
):
    hbm = pl.BlockSpec(memory_space=pltpu.HBM)

    def vmem(*shape, dtype=BF16):
        return pltpu.VMEM(shape, dtype)

    def dma(*shape):
        return pltpu.SemaphoreType.DMA(shape)

    scratch = [
        vmem(SEQ, D), vmem(SEQ, LC, dtype=F32), vmem(3, SEQ, LC), vmem(4, LC), vmem(4, 1, D, dtype=F32),
        vmem(1, LC, dtype=F32), vmem(D, LC), vmem(D, LC), vmem(4, 128, 128), vmem(4, 128, 128), vmem(LC, D),
        vmem(TOP, SEQ, dtype=jnp.int32), vmem(TOP, SEQ, dtype=F32),
        vmem(1, D, HID), vmem(1, D, HID), vmem(2, HID, HALF), vmem(D, HID), vmem(D, HID), vmem(HID, D),
        vmem(SEQ, D), vmem(SEQ, D),
        vmem(2, SEQ, HALF), vmem(2, SEQ, HALF), vmem(2 * TOP, NZ * SEQ, dtype=F32), vmem(NZ, 2 * TOP, NZ * SEQ, dtype=F32),
        vmem(SEQ, D), vmem(SEQ, D),
        vmem(NCH, NZ * SEQ, CW), vmem(NCH, NQ * ROWS, CW), vmem(2, NCH, NQ * ROWS, CW),
        vmem(NQ * ROWS, NZ * SEQ), vmem(NZ * SEQ, NQ * ROWS), vmem(NZ * SEQ, NQ * ROWS), vmem(NQ * ROWS, HID),
        vmem(NCH, NQ * ROWS, CW), vmem(NCH, NQ * ROWS, CW), vmem(NCH, NQ * ROWS, CW), vmem(NCH, NQ * ROWS, CW),
        vmem(NCH, NZ * SEQ, CW), vmem(NCH, 2, 2, SEQ, CW), vmem(NCH, 2, SEQ, CW), vmem(NCH, 4, SEQ, CW),
        vmem(2, NCH, SEQ, CW),
        dma(29),
        dma(3), dma(3), pltpu.SemaphoreType.DMA, pltpu.SemaphoreType.DMA, dma(NCH), dma(NCH, 2), dma(NCH), dma(NCH),
        dma(NCH), dma(NCH), dma(NCH), dma(NCH), dma(NCH), dma(NCH), dma(NCH), dma(NCH), dma(NCH, 2), dma(NCH), dma(NCH),
        dma(NCH),
    ]
    vm = pl.BlockSpec(memory_space=pltpu.VMEM)
    results = pl.pallas_call(
        kernel,
        out_shape=(
            pltpu.VMEM((SEQ, D), BF16),
            pltpu.VMEM((SEQ, LC), F32),
            pltpu.VMEM((3, SEQ, LC), BF16),
        ),
        in_specs=[hbm] * 22,
        out_specs=(vm,) * 3,
        scratch_shapes=scratch,
        compiler_params=pltpu.CompilerParams(collective_id=0, has_side_effects=True, vmem_limit_bytes=60 * 2**20),
        name="layer",
    )(
        tokens, lru_state, conv_window.transpose(1, 0, 2), conv_taps, gain_mix_in[None], gain_mix_out[None],
        gain_ffn_in[None], gain_ffn_out[None], decay_rate[None], w_branch, w_input, gate_a, gate_x, w_mix_out,
        routes.T, route_weight.T, expert_gate, expert_up, expert_down[0], shared_gate, shared_up, shared_down,
    )
    layer_out, new_state, window = pl.pallas_call(
        store,
        out_shape=tuple(jax.ShapeDtypeStruct(r.shape, r.dtype) for r in results),
        in_specs=[vm] * 3,
        out_specs=(hbm,) * 3,
        scratch_shapes=[dma(3)],
        compiler_params=pltpu.CompilerParams(has_side_effects=True, vmem_limit_bytes=2**20),
        name="store",
    )(*results)
    return (layer_out, new_state, window.transpose(1, 0, 2))


def solution(mesh):
    placed = (
        P("ep", None),
        P("ep", "tp"),
        P("ep", None, "tp"),
        P(),
        P(),
        P(),
        P(),
        P(None, "tp"),
        P(None, "tp"),
        P(None, "tp"),
        P("tp", None, None),
        P("tp", None, None),
        P("tp"),
        P("tp", None),
        P("ep", None),
        P("ep", None),
        P("ep", None, "tp"),
        P("ep", None, "tp"),
        P("ep", "tp", None),
        P(None, "tp"),
        P(None, "tp"),
        P("tp", None),
    )
    return jax.shard_map(
        on_device,
        mesh=mesh,
        in_specs=placed,
        out_specs=(P("ep", None), P("ep", "tp"), P("ep", None, "tp")),
        check_vma=False,
    )
```

```python
import functools

import jax
import jax.numpy as jnp
from jax import lax
from jax.experimental import pallas as pl
from jax.experimental.pallas import tpu as pltpu
from jax.sharding import PartitionSpec as P

MESH = pl.DeviceIdType.MESH
F32 = jnp.float32
BF16 = jnp.bfloat16

NZ = 8
NQ = 16
SEQ = 32
TOP = 4
D = 2048
HALF = D // 2
WIDTHS = (256, 384, 256, 128)
NCH = len(WIDTHS)
STARTS = tuple(sum(WIDTHS[:i]) for i in range(NCH))
FAR = (10, 11, 9, 14, 6, 15, 5, 13, 7, 2, 8, 3, 1, 12, 4)
LC = 512
HID = 256
ROWS = NZ * 2
NPIECE = 4


def scaled(value, gain):
    return value * lax.rsqrt(jnp.mean(value * value, axis=-1, keepdims=True) + 1e-06) * gain


def dot(a, b):
    return jnp.dot(a, b, preferred_element_type=F32)


def kernel(
    tok_h, lru_h, win_h, taps_h, gain0_h, gain1_h, gain2_h, gain3_h, decay_h, wb_h, wi_h, ga_h, gx_h, wm_h,
    routes_h, rweight_h, eg_h, eu_h, ed_h, sg_h, su_h, sd_h,
    out_v, state_v, window_v,
    tok, lru, win, taps, gains, decay, wb, wi, ga, gx, wm, routes, rweight,
    eg, eu, ed, sg, su, sd,
    middle_v, ffn,
    mix_s, mix_r, meta_s, meta_r, sh_s, sh_r,
    g_buf, r_buf, x_buf, p_buf, whi, wlo, hid_v, y_s, y_r, o_buf, b_buf, t_buf, rl_buf, c_buf, v_buf, rt_buf,
    lsem,
    tp_s, tp_r, ms_s, ms_r, za_s, za_two, za_r, xa_s, xa_r, xf_s, xf_r, yx_s, yx_r, xb_s, xb_r,
    zb_s, zb_two, zb_r, rt_s, rt_r,
):
    me = lax.axis_index("ep")
    c = lax.axis_index("tp")
    z = me // NQ
    q = me % NQ
    y, x = q // 4, q % 4

    def z_peer(i):
        return lax.rem(z + (i + NZ), NZ)

    y_peer = [lax.rem(y + i, 4) * 4 for i in range(4)]
    x_peer = [lax.rem(x + i, 4) for i in range(4)]

    def q_peer(i):
        return y_peer[i // 4] + x_peer[i % 4]

    def rows(i, n):
        return pl.ds(pl.multiple_of(i * n, n), n)

    def load(k, src, dst):
        copy = pltpu.make_async_copy(src, dst, lsem.at[k])
        copy.start()
        return copy

    step = D // NPIECE
    l_tok = load(0, tok_h, tok)
    l_gains = [load(1, gain0_h, gains.at[0])]
    l_wi = [load(5 + i, wi_h.at[pl.ds(i * step, step)], wi.at[pl.ds(i * step, step)]) for i in range(NPIECE)]
    l_win = load(9, win_h, win)
    l_taps = load(10, taps_h, taps)
    l_ga = load(11, ga_h, ga)
    l_gx = load(12, gx_h, gx)
    l_decay = load(19, decay_h, decay)
    l_lru = load(20, lru_h, lru)
    l_wb = [load(15 + i, wb_h.at[pl.ds(i * step, step)], wb.at[pl.ds(i * step, step)]) for i in range(NPIECE)]
    l_wm = [load(21 + i, wm_h.at[:, pl.ds(i * HALF, HALF)], wm.at[i]) for i in range(2)]
    l_routes = load(13, routes_h, routes)
    l_rweight = load(14, rweight_h, rweight)
    l_gains += [load(1 + i, h, gains.at[i]) for i, h in ((1, gain1_h), (2, gain2_h), (3, gain3_h))]

    barrier = pltpu.get_barrier_semaphore()
    pl.semaphore_signal(barrier, inc=1, device_id=(me, 1 - c), device_id_type=MESH)

    def greet_z(i, carry):
        pl.semaphore_signal(barrier, inc=1, device_id=(z_peer(i) * NQ + q, c), device_id_type=MESH)
        return carry

    lax.fori_loop(1, NZ, greet_z, 0)
    for i in FAR:
        pl.semaphore_signal(barrier, inc=1, device_id=(z * NQ + q_peer(i), c), device_id_type=MESH)

    l_tok.wait()
    l_gains[0].wait()
    normed = scaled(tok[...].astype(F32), gains[0]).astype(BF16)
    inflow = jnp.zeros((SEQ, LC), F32)
    for i in range(NPIECE):
        l_wi[i].wait()
        inflow += dot(normed[:, i * step : (i + 1) * step], wi[i * step : (i + 1) * step, :])
    inflow = inflow.astype(BF16)
    l_win.wait()
    l_taps.wait()
    conv = inflow.astype(F32) * taps[3:4, :].astype(F32)
    for j in range(3):
        conv += win[j].astype(F32) * taps[j : j + 1, :].astype(F32)
        window_v[j] = win[j + 1] if j < 2 else inflow
    low = conv.astype(BF16)
    l_ga.wait()
    l_gx.wait()
    groups = LC // 128
    recur = [dot(low[:, g * 128 : (g + 1) * 128], ga[g]) for g in range(groups)]
    inputs = [dot(low[:, g * 128 : (g + 1) * 128], gx[g]) for g in range(groups)]
    recur_gate = jax.nn.sigmoid(jnp.concatenate(recur, axis=1))
    input_gate = jax.nn.sigmoid(jnp.concatenate(inputs, axis=1))
    l_decay.wait()
    l_lru.wait()
    fall = 8.0 * recur_gate * decay[...]
    t = jnp.tanh(fall)
    state = jnp.exp(-fall) * lru[...] + jnp.sqrt(2.0 * t / (1.0 + t)) * conv * input_gate
    state_v[...] = state
    branch = jnp.zeros((SEQ, LC), F32)
    for i in range(NPIECE):
        l_wb[i].wait()
        branch += dot(normed[:, i * step : (i + 1) * step], wb[i * step : (i + 1) * step, :])
    gated = (state * jax.nn.gelu(branch)).astype(BF16)
    for i in range(2):
        l_wm[i].wait()
        mix_s[i] = dot(gated, wm[i]).astype(BF16)

    l_sg = load(23, sg_h, sg)
    l_su = load(24, su_h, su)
    l_sd = load(25, sd_h, sd)
    l_eg = load(26, eg_h, eg)
    l_eu = load(27, eu_h, eu)
    l_ed = [load(28 + i, ed_h.at[:, pl.ds(i * HALF, HALF)], ed.at[i]) for i in range(2)]

    pl.semaphore_wait(barrier, 1 + (NZ - 1) + (NQ - 1))

    def remote(src, dst, ssem, rsem, e, t):
        return pltpu.make_async_remote_copy(
            src_ref=src, dst_ref=dst, send_sem=ssem, recv_sem=rsem, device_id=(e, t), device_id_type=MESH
        )

    def to_z(src, dst, ssem, rsem, i):
        return remote(src, dst, ssem, rsem, z_peer(i) * NQ + q, c)

    def to_core(src, dst, ssem, rsem):
        return remote(src, dst, ssem, rsem, me, 1 - c)

    mix_copies = [to_core(mix_s.at[i], mix_r.at[i], tp_s.at[i], tp_r.at[i]) for i in range(2)]
    for copy in mix_copies:
        copy.start()

    with jax.named_scope("slots"):
        l_routes.wait()
        l_rweight.wait()
        lane = lax.broadcasted_iota(jnp.int32, (1, NZ * SEQ), 1)
        mine = (lane // SEQ) == z
        earlier = lax.broadcasted_iota(jnp.int32, (SEQ, NZ * SEQ), 0) < (lane % SEQ)
        diagonal = lax.broadcasted_iota(jnp.int32, (SEQ, SEQ), 0) == lax.broadcasted_iota(jnp.int32, (SEQ, SEQ), 1)
        narrow = routes[...].astype(F32)
        named = [
            jnp.sum(jnp.where(diagonal, narrow[k : k + 1, :], 0.0), axis=1, keepdims=True) for k in range(TOP)
        ]
        wide = jnp.concatenate([narrow] * NZ, axis=1)
        for k in range(TOP):
            expert = wide[k : k + 1, :]
            same = named[0] == expert
            for j in range(1, TOP):
                same = same | (named[j] == expert)
            rank = jnp.sum(jnp.where(same & earlier, 1.0, 0.0), axis=0, keepdims=True)
            meta_s[k : k + 1, :] = jnp.where(mine, 2.0 * expert + rank, 0.0)
        meta_s[TOP : 2 * TOP, :] = jnp.where(mine, jnp.concatenate([rweight[...]] * NZ, axis=1), 0.0)
        meta_r[pl.ds(z, 1)] = meta_s[...][None]

    def meta_send(i, carry):
        to_z(meta_s, meta_r.at[z], ms_s, ms_r, i).start()
        return carry

    lax.fori_loop(1, NZ, meta_send, 0)

    for copy in l_gains[1:]:
        copy.wait()
    mixed = []
    for i in range(2):
        mix_copies[i].wait()
        mixed.append(mix_s[i].astype(F32) + mix_r[i].astype(F32))
    mixed = jnp.concatenate(mixed, axis=1)
    middle = (tok[...].astype(F32) + scaled(mixed, gains[1])).astype(BF16)
    middle_v[...] = middle
    ffn[...] = scaled(middle.astype(F32), gains[2]).astype(BF16)

    def z_copy(ch, source, i, rsem):
        block = g_buf[ch].at[rows(source, SEQ)]
        return to_z(block, block, za_s.at[ch], rsem, i)

    def direct(ch):
        columns = pl.ds(pl.multiple_of(c * HALF + STARTS[ch], 128), WIDTHS[ch])
        g_buf[ch][rows(z, SEQ), :] = ffn[:, columns]
        z_copy(ch, z, 2, za_two.at[ch, 0]).start()
        z_copy(ch, z, -2, za_two.at[ch, 1]).start()
        z_copy(ch, z, 1, za_r.at[ch]).start()
        z_copy(ch, z, -1, za_r.at[ch]).start()

    def relay(ch):
        for way in range(2):
            sign = 1 - 2 * way
            source = z_peer(-2 * sign)
            z_copy(ch, source, sign, za_two.at[ch, way]).wait_recv()
            if ch % 2 == way:
                z_copy(ch, source, 2 * sign, za_r.at[ch]).start()
            z_copy(ch, source, sign, za_r.at[ch]).start()

    for ch in range(NCH - 1):
        direct(ch)

    l_sg.wait()
    l_su.wait()
    l_sd.wait()
    hidden = (jax.nn.silu(dot(ffn[...], sg[...])) * dot(ffn[...], su[...])).astype(BF16)
    sh_s[...] = dot(hidden, sd[...]).astype(BF16)
    sh_copy = to_core(sh_s, sh_r, tp_s.at[2], tp_r.at[2])
    sh_copy.start()

    relay(0)
    direct(NCH - 1)
    relay(1)

    many = meta_r.at[pl.ds(0, NZ - 1)]
    to_z(many, many, ms_s, ms_r, 1).wait()
    meta = jnp.sum(meta_r[...], axis=0)
    code = meta[0:TOP, :].astype(jnp.int32)
    place = ((code % (2 * NQ)) // 2) * ROWS + (lane // SEQ) * 2 + code % 2
    place = jnp.where(code // (2 * NQ) == z, place, -1)
    row = lax.broadcasted_iota(jnp.int32, (NQ * ROWS, NZ * SEQ), 0)
    filled = jnp.zeros((NQ * ROWS, NZ * SEQ), F32)
    weight = jnp.zeros((NQ * ROWS, NZ * SEQ), F32)
    for k in range(TOP):
        hit = row == place[k : k + 1, :]
        filled = jnp.where(hit, 1.0, filled)
        weight = jnp.where(hit, meta[TOP + k : TOP + k + 1, :], weight)
    p_buf[...] = filled.astype(BF16)
    weight = weight.T
    high = weight.astype(BF16)
    whi[...] = high
    wlo[...] = (weight - high.astype(F32)).astype(BF16)

    def q_send(src, dst, ssem, rsem):
        for i in FAR:
            p = q_peer(i)
            remote(src.at[rows(p, ROWS)], dst.at[rows(q, ROWS)], ssem, rsem, z * NQ + p, c).start()

    def q_all(buf, ssem, rsem):
        part = buf.at[pl.ds(0, (NQ - 1) * ROWS)]
        return remote(part, part, ssem, rsem, z * NQ + q_peer(1), c)

    def picked(ch):
        part = g_buf[ch].at[pl.ds(0, 5 * SEQ)]
        to_z(part, part, za_s.at[ch], za_r.at[ch], 1).wait_recv()
        r_buf[ch][...] = dot(p_buf[...], g_buf[ch][...]).astype(BF16)
        q_send(r_buf[ch], x_buf[ch].at[c], xa_s.at[ch], xa_r.at[ch])
        x_buf[ch][c, rows(q, ROWS), :] = r_buf[ch][rows(q, ROWS), :]

    relay(2)
    picked(0)
    relay(3)
    picked(1)
    picked(2)
    picked(3)

    l_eg.wait()
    l_eu.wait()
    gate = jnp.zeros((NQ * ROWS, HID), F32)
    up = jnp.zeros((NQ * ROWS, HID), F32)
    forwards = []
    for ch in range(NCH):
        q_all(x_buf[ch].at[c], xa_s.at[ch], xa_r.at[ch]).wait_recv()
        copy = to_core(x_buf[ch].at[c], x_buf[ch].at[c], xf_s.at[ch], xf_r.at[ch])
        copy.start()
        forwards.append(copy)
        depth = pl.ds(pl.multiple_of(c * HALF + STARTS[ch], 128), WIDTHS[ch])
        gate += dot(x_buf[ch][c], eg[0, depth, :])
        up += dot(x_buf[ch][c], eu[0, depth, :])
    for ch in range(NCH):
        other = to_core(x_buf[ch].at[1 - c], x_buf[ch].at[1 - c], xf_s.at[ch], xf_r.at[ch])
        other.wait_recv()
        depth = pl.ds(pl.multiple_of((1 - c) * HALF + STARTS[ch], 128), WIDTHS[ch])
        gate += dot(x_buf[ch][1 - c], eg[0, depth, :])
        up += dot(x_buf[ch][1 - c], eu[0, depth, :])
    hid_v[...] = (jax.nn.silu(gate) * up).astype(BF16)

    for copy in l_ed:
        copy.wait()
    trades = []

    def down(core, ch):
        return dot(hid_v[...], ed[core, :, STARTS[ch] : STARTS[ch] + WIDTHS[ch]]).astype(BF16)

    def trade(ch):
        y_s[ch][...] = down(1 - c, ch)
        copy = to_core(y_s[ch], y_r[ch], yx_s.at[ch], yx_r.at[ch])
        copy.start()
        trades.append(copy)

    def back(ch):
        own = down(c, ch).astype(F32)
        trades[ch].wait()
        o_buf[ch][...] = (own + y_r[ch][...].astype(F32)).astype(BF16)
        q_send(o_buf[ch], b_buf[ch], xb_s.at[ch], xb_r.at[ch])
        b_buf[ch][rows(q, ROWS), :] = o_buf[ch][rows(q, ROWS), :]

    trade(0)
    trade(1)
    back(0)
    trade(2)
    back(1)
    trade(3)
    back(2)
    back(3)

    def weighted(ch):
        q_all(b_buf[ch], xb_s.at[ch], xb_r.at[ch]).wait_recv()
        t_buf[ch][...] = (dot(whi[...], b_buf[ch][...]) + dot(wlo[...], b_buf[ch][...])).astype(BF16)
        sem = zb_s.at[ch]
        if ch == NCH - 1:
            for slot, i in enumerate((4, 3, -3, 2, -2, 1, -1)):
                to_z(t_buf[ch].at[rows(z_peer(i), SEQ)], v_buf[ch].at[slot], sem, zb_r.at[ch], i).start()
            return
        for way in range(2):
            sign = 1 - 2 * way
            two = zb_two.at[ch, way]
            if ch % 2 == way:
                to_z(t_buf[ch].at[rows(z_peer(4), SEQ)], rl_buf[ch].at[way, 1], sem, two, -2 * sign).start()
            to_z(t_buf[ch].at[rows(z_peer(-3 * sign), SEQ)], rl_buf[ch].at[way, 0], sem, two, -sign).start()
        for way in range(2):
            sign = 1 - 2 * way
            to_z(t_buf[ch].at[rows(z_peer(-sign), SEQ)], v_buf[ch].at[way], sem, zb_r.at[ch], -sign).start()

    def relayed(ch):
        for way in range(2):
            sign = 1 - 2 * way
            many = rl_buf[ch].at[way, pl.ds(0, 2 if ch % 2 == way else 1)]
            to_z(many, many, zb_s.at[ch], zb_two.at[ch, way], 1).wait_recv()
            total = t_buf[ch][rows(z_peer(-2 * sign), SEQ), :].astype(F32) + rl_buf[ch][way, 0].astype(F32)
            if ch % 2 == way:
                total += rl_buf[ch][way, 1].astype(F32)
            c_buf[ch][way] = total.astype(BF16)
            to_z(c_buf[ch].at[way], v_buf[ch].at[2 + way], zb_s.at[ch], zb_r.at[ch], -2 * sign).start()

    weighted(0)
    weighted(1)
    relayed(0)
    weighted(2)
    relayed(1)
    weighted(3)
    relayed(2)

    sh_copy.wait()
    shared = sh_s[...].astype(F32) + sh_r[...].astype(F32)
    pairs = []
    for ch in range(NCH):
        to_z(v_buf[ch], v_buf[ch], zb_s.at[ch], zb_r.at[ch], 1).wait_recv()
        total = t_buf[ch][rows(z, SEQ), :].astype(F32)
        for s in range(7 if ch == NCH - 1 else 4):
            total += v_buf[ch][s].astype(F32)
        rt_buf[ch][c] = total.astype(BF16)
        copy = to_core(rt_buf[ch].at[c], rt_buf[ch].at[c], rt_s.at[ch], rt_r.at[ch])
        copy.start()
        pairs.append(copy)

    for ch in range(NCH):
        for buf, sem in ((g_buf, za_s), (t_buf, zb_s)):
            part = buf[ch].at[pl.ds(0, 7 * SEQ)]
            to_z(part, part, sem.at[ch], za_r.at[ch], 1).wait_send()
        q_all(r_buf[ch], xa_s.at[ch], xa_r.at[ch]).wait_send()
        q_all(o_buf[ch], xb_s.at[ch], xb_r.at[ch]).wait_send()
        forwards[ch].wait_send()
    for ch in range(NCH):
        to_core(rt_buf[ch].at[1 - c], rt_buf[ch].at[1 - c], rt_s.at[ch], rt_r.at[ch]).wait_recv()
    routed = jnp.concatenate([rt_buf[ch][h] for h in range(2) for ch in range(NCH)], axis=1)
    last = scaled(routed.astype(F32) + shared, gains[3])
    out_v[...] = (middle_v[...].astype(F32) + last).astype(BF16)
    for copy in pairs:
        copy.wait_send()


def store(*refs):
    n = len(refs) // 2
    copies = [pltpu.make_async_copy(refs[i], refs[n + i], refs[-1].at[i]) for i in range(n)]
    for copy in copies:
        copy.start()
    for copy in copies:
        copy.wait()


def on_device(
    tokens, lru_state, conv_window, gain_mix_in, gain_mix_out, gain_ffn_in, gain_ffn_out, w_branch, w_input,
    conv_taps, gate_a, gate_x, decay_rate, w_mix_out, routes, route_weight, expert_gate, expert_up, expert_down,
    shared_gate, shared_up, shared_down,
):
    hbm = pl.BlockSpec(memory_space=pltpu.HBM)

    def vmem(*shape, dtype=BF16):
        return pltpu.VMEM(shape, dtype)

    def chunks(*shape):
        return [vmem(*shape, width) for width in WIDTHS]

    def dma(*shape):
        return pltpu.SemaphoreType.DMA(shape)

    scratch = [
        vmem(SEQ, D), vmem(SEQ, LC, dtype=F32), vmem(3, SEQ, LC), vmem(4, LC), vmem(4, 1, D, dtype=F32),
        vmem(1, LC, dtype=F32), vmem(D, LC), vmem(D, LC), vmem(4, 128, 128), vmem(4, 128, 128), vmem(2, LC, HALF),
        vmem(TOP, SEQ, dtype=jnp.int32), vmem(TOP, SEQ, dtype=F32),
        vmem(1, D, HID), vmem(1, D, HID), vmem(2, HID, HALF), vmem(D, HID), vmem(D, HID), vmem(HID, D),
        vmem(SEQ, D), vmem(SEQ, D),
        vmem(2, SEQ, HALF), vmem(2, SEQ, HALF), vmem(2 * TOP, NZ * SEQ, dtype=F32), vmem(NZ, 2 * TOP, NZ * SEQ, dtype=F32),
        vmem(SEQ, D), vmem(SEQ, D),
        chunks(NZ * SEQ), chunks(NQ * ROWS), chunks(2, NQ * ROWS),
        vmem(NQ * ROWS, NZ * SEQ), vmem(NZ * SEQ, NQ * ROWS), vmem(NZ * SEQ, NQ * ROWS), vmem(NQ * ROWS, HID),
        chunks(NQ * ROWS), chunks(NQ * ROWS), chunks(NQ * ROWS), chunks(NQ * ROWS),
        chunks(NZ * SEQ), chunks(2, 2, SEQ), chunks(2, SEQ),
        [vmem(7 if ch == NCH - 1 else 4, SEQ, WIDTHS[ch]) for ch in range(NCH)], chunks(2, SEQ),
        dma(30),
        dma(3), dma(3), pltpu.SemaphoreType.DMA, pltpu.SemaphoreType.DMA, dma(NCH), dma(NCH, 2), dma(NCH), dma(NCH),
        dma(NCH), dma(NCH), dma(NCH), dma(NCH), dma(NCH), dma(NCH), dma(NCH), dma(NCH), dma(NCH, 2), dma(NCH), dma(NCH),
        dma(NCH),
    ]
    vm = pl.BlockSpec(memory_space=pltpu.VMEM)
    results = pl.pallas_call(
        kernel,
        out_shape=(
            pltpu.VMEM((SEQ, D), BF16),
            pltpu.VMEM((SEQ, LC), F32),
            pltpu.VMEM((3, SEQ, LC), BF16),
        ),
        in_specs=[hbm] * 22,
        out_specs=(vm,) * 3,
        scratch_shapes=scratch,
        compiler_params=pltpu.CompilerParams(collective_id=0, has_side_effects=True, vmem_limit_bytes=60 * 2**20),
        name="layer",
    )(
        tokens, lru_state, conv_window.transpose(1, 0, 2), conv_taps, gain_mix_in[None], gain_mix_out[None],
        gain_ffn_in[None], gain_ffn_out[None], decay_rate[None], w_branch, w_input, gate_a, gate_x, w_mix_out,
        routes.T, route_weight.T, expert_gate, expert_up, expert_down[0], shared_gate, shared_up, shared_down,
    )
    layer_out, new_state, window = pl.pallas_call(
        store,
        out_shape=tuple(jax.ShapeDtypeStruct(r.shape, r.dtype) for r in results),
        in_specs=[vm] * 3,
        out_specs=(hbm,) * 3,
        scratch_shapes=[dma(3)],
        compiler_params=pltpu.CompilerParams(has_side_effects=True, vmem_limit_bytes=2**20),
        name="store",
    )(*results)
    return (layer_out, new_state, window.transpose(1, 0, 2))


def solution(mesh):
    placed = (
        P("ep", None),
        P("ep", "tp"),
        P("ep", None, "tp"),
        P(),
        P(),
        P(),
        P(),
        P(None, "tp"),
        P(None, "tp"),
        P(None, "tp"),
        P("tp", None, None),
        P("tp", None, None),
        P("tp"),
        P("tp", None),
        P("ep", None),
        P("ep", None),
        P("ep", None, "tp"),
        P("ep", None, "tp"),
        P("ep", "tp", None),
        P(None, "tp"),
        P(None, "tp"),
        P("tp", None),
    )
    return jax.shard_map(
        on_device,
        mesh=mesh,
        in_specs=placed,
        out_specs=(P("ep", None), P("ep", "tp"), P("ep", None, "tp")),
        check_vma=False,
    )
```

```python
import functools

import jax
import jax.numpy as jnp
from jax import lax
from jax.experimental import pallas as pl
from jax.experimental.pallas import tpu as pltpu
from jax.sharding import PartitionSpec as P

MESH = pl.DeviceIdType.MESH
F32 = jnp.float32
BF16 = jnp.bfloat16

NZ = 8
NQ = 16
SEQ = 32
TOP = 4
D = 2048
HALF = D // 2
WIDTHS = (256, 512, 256)
NCH = len(WIDTHS)
STARTS = tuple(sum(WIDTHS[:i]) for i in range(NCH))
FAR = (10, 11, 9, 14, 6, 15, 5, 13, 7, 2, 8, 3, 1, 12, 4)
LC = 512
HID = 256
ROWS = NZ * 2
NLOAD = 20
PLUS = (0, 1, 0)
PIECES = ((0, 768), (768, 768), (1536, 512))


def scaled(value, gain):
    return value * lax.rsqrt(jnp.mean(value * value, axis=-1, keepdims=True) + 1e-06) * gain


def dot(a, b):
    return jnp.dot(a, b, preferred_element_type=F32)


def kernel(
    tok_h, lru_h, win_h, taps_h, gain0_h, gain1_h, gain2_h, gain3_h, decay_h, wb_h, wi_h, ga_h, gx_h, wm_h,
    routes_h, rweight_h, eg_h, eu_h, ed_h, sg_h, su_h, sd_h,
    out_v, state_v, window_v,
    tok, lru, win, taps, gains, decay, wb, wi, gax, wm, routes, rweight,
    egu, ed, sgu, sd,
    middle_v, ffn,
    mix_s, mix_r, meta_s, meta_r, sh_s, sh_r,
    g_buf, r_buf, x_buf, p_buf, whi, wlo, hid_v, y_s, y_r, o_buf, b_buf, t_buf, rl_buf, c_buf, v_buf, rt_buf,
    lsem, core_s, chip_s, meta_sem, mix_r_sem, sh_r_sem, rt_r_sem,
    za_two, za_r, xa_r, xf_r, yx_r, xb_r, zb_two, zb_r,
):
    me = lax.axis_index("ep")
    c = lax.axis_index("tp")
    z = me // NQ
    q = me % NQ
    y, x = q // 4, q % 4

    def z_peer(i):
        return lax.rem(z + (i + NZ), NZ)

    y_peer = [lax.rem(y + i, 4) * 4 for i in range(4)]
    x_peer = [lax.rem(x + i, 4) for i in range(4)]

    def q_peer(i):
        return y_peer[i // 4] + x_peer[i % 4]

    def rows(i, n):
        return pl.ds(pl.multiple_of(i * n, n), n)

    count = iter(range(NLOAD))

    def load(*pairs):
        k = next(count)
        copies = [pltpu.make_async_copy(src, dst, lsem.at[k]) for src, dst in pairs]
        for copy in copies:
            copy.start()
        return k, copies[0]

    def loaded(group, whole=None):
        k, copy = group
        if whole is not None:
            copy = pltpu.make_async_copy(whole, whole, lsem.at[k])
        copy.wait()

    l_tok = load((tok_h, tok))
    l_gain0 = load((gain0_h, gains.at[0]))
    l_wi = [load((wi_h.at[pl.ds(i, n)], wi.at[pl.ds(i, n)])) for i, n in PIECES]
    l_win = load((win_h, win))
    l_taps = load((taps_h, taps))
    l_gax = load((ga_h, gax.at[0]), (gx_h, gax.at[1]))
    l_decay = load((decay_h, decay))
    l_lru = load((lru_h, lru))
    l_wb = load((wb_h, wb))
    l_wm = [load((wm_h.at[:, pl.ds(i * HALF, HALF)], wm.at[i])) for i in range(2)]
    l_routes = load((routes_h, routes))
    l_rweight = load((rweight_h, rweight))
    l_gains = load((gain1_h, gains.at[1]), (gain2_h, gains.at[2]), (gain3_h, gains.at[3]))

    barrier = pltpu.get_barrier_semaphore()
    pl.semaphore_signal(barrier, inc=1, device_id=(me, 1 - c), device_id_type=MESH)

    def greet_z(i, carry):
        pl.semaphore_signal(barrier, inc=1, device_id=(z_peer(i) * NQ + q, c), device_id_type=MESH)
        return carry

    lax.fori_loop(1, NZ, greet_z, 0)
    for i in FAR:
        pl.semaphore_signal(barrier, inc=1, device_id=(z * NQ + q_peer(i), c), device_id_type=MESH)

    loaded(l_tok)
    loaded(l_gain0)
    normed = scaled(tok[...].astype(F32), gains[0]).astype(BF16)
    inflow = jnp.zeros((SEQ, LC), F32)
    for group, (i, n) in zip(l_wi, PIECES):
        loaded(group)
        inflow += dot(normed[:, i : i + n], wi[i : i + n, :])
    inflow = inflow.astype(BF16)
    loaded(l_win)
    loaded(l_taps)
    conv = inflow.astype(F32) * taps[3:4, :].astype(F32)
    for j in range(3):
        conv += win[j].astype(F32) * taps[j : j + 1, :].astype(F32)
        window_v[j] = win[j + 1] if j < 2 else inflow
    low = conv.astype(BF16)
    loaded(l_gax, gax)
    loaded(l_decay)
    loaded(l_lru)
    loaded(l_wb)
    branch = dot(normed, wb[...])
    groups = LC // 128
    recur = [dot(low[:, g * 128 : (g + 1) * 128], gax[0, g]) for g in range(groups)]
    inputs = [dot(low[:, g * 128 : (g + 1) * 128], gax[1, g]) for g in range(groups)]
    recur_gate = jax.nn.sigmoid(jnp.concatenate(recur, axis=1))
    input_gate = jax.nn.sigmoid(jnp.concatenate(inputs, axis=1))
    fall = 8.0 * recur_gate * decay[...]
    t = jnp.tanh(fall)
    state = jnp.exp(-fall) * lru[...] + jnp.sqrt(2.0 * t / (1.0 + t)) * conv * input_gate
    state_v[...] = state
    gated = (state * jax.nn.gelu(branch)).astype(BF16)
    for i in range(2):
        loaded(l_wm[i])
        mix_s[i] = dot(gated, wm[i]).astype(BF16)

    l_sgu = load((sg_h, sgu.at[0]), (su_h, sgu.at[1]))
    l_sd = load((sd_h, sd))
    l_egu = load((eg_h.at[0], egu.at[0]), (eu_h.at[0], egu.at[1]))
    l_ed = load(*[(ed_h.at[:, pl.ds(i * HALF, HALF)], ed.at[i]) for i in range(2)])

    pl.semaphore_wait(barrier, 1 + (NZ - 1) + (NQ - 1))

    def remote(src, dst, ssem, rsem, e, t):
        return pltpu.make_async_remote_copy(
            src_ref=src, dst_ref=dst, send_sem=ssem, recv_sem=rsem, device_id=(e, t), device_id_type=MESH
        )

    def to_z(src, dst, rsem, i):
        return remote(src, dst, chip_s, rsem, z_peer(i) * NQ + q, c)

    def to_core(src, dst, rsem):
        return remote(src, dst, core_s, rsem, me, 1 - c)

    def arrived(ref, rsem):
        to_core(ref, ref, rsem).wait_recv()

    mix_copies = [to_core(mix_s.at[i], mix_r.at[i], mix_r_sem.at[i]) for i in range(2)]
    for copy in mix_copies:
        copy.start()

    with jax.named_scope("slots"):
        loaded(l_routes)
        loaded(l_rweight)
        lane = lax.broadcasted_iota(jnp.int32, (1, NZ * SEQ), 1)
        mine = (lane // SEQ) == z
        earlier = lax.broadcasted_iota(jnp.int32, (SEQ, NZ * SEQ), 0) < (lane % SEQ)
        diagonal = lax.broadcasted_iota(jnp.int32, (SEQ, SEQ), 0) == lax.broadcasted_iota(jnp.int32, (SEQ, SEQ), 1)
        narrow = routes[...].astype(F32)
        named = [
            jnp.sum(jnp.where(diagonal, narrow[k : k + 1, :], 0.0), axis=1, keepdims=True) for k in range(TOP)
        ]
        wide = jnp.concatenate([narrow] * NZ, axis=1)
        for k in range(TOP):
            expert = wide[k : k + 1, :]
            same = named[0] == expert
            for j in range(1, TOP):
                same = same | (named[j] == expert)
            rank = jnp.sum(jnp.where(same & earlier, 1.0, 0.0), axis=0, keepdims=True)
            meta_s[k : k + 1, :] = jnp.where(mine, 2.0 * expert + rank, 0.0)
        meta_s[TOP : 2 * TOP, :] = jnp.where(mine, jnp.concatenate([rweight[...]] * NZ, axis=1), 0.0)
        meta_r[pl.ds(z, 1)] = meta_s[...][None]

    def meta_send(i, carry):
        remote(meta_s, meta_r.at[z], meta_sem.at[0], meta_sem.at[1], z_peer(i) * NQ + q, c).start()
        return carry

    lax.fori_loop(1, NZ, meta_send, 0)

    loaded(l_gains, gains.at[pl.ds(1, 3)])
    mixed = []
    for i in range(2):
        mix_copies[i].wait_recv()
        mixed.append(mix_s[i].astype(F32) + mix_r[i].astype(F32))
    mixed = jnp.concatenate(mixed, axis=1)
    middle = (tok[...].astype(F32) + scaled(mixed, gains[1])).astype(BF16)
    middle_v[...] = middle
    ffn[...] = scaled(middle.astype(F32), gains[2]).astype(BF16)

    def z_copy(ch, source, i, rsem):
        block = g_buf[ch].at[rows(source, SEQ)]
        return to_z(block, block, rsem, i)

    def direct(ch):
        columns = pl.ds(pl.multiple_of(c * HALF + STARTS[ch], 128), WIDTHS[ch])
        g_buf[ch][rows(z, SEQ), :] = ffn[:, columns]
        z_copy(ch, z, 2, za_two.at[ch]).start()
        z_copy(ch, z, -2, za_two.at[ch]).start()
        z_copy(ch, z, 1, za_r.at[ch]).start()
        z_copy(ch, z, -1, za_r.at[ch]).start()

    def relay(ch):
        arrived(g_buf[ch].at[pl.ds(0, 2 * SEQ)], za_two.at[ch])
        for way in range(2):
            sign = 1 - 2 * way
            source = z_peer(-2 * sign)
            if PLUS[ch] == way:
                z_copy(ch, source, 2 * sign, za_r.at[ch]).start()
            z_copy(ch, source, sign, za_r.at[ch]).start()

    for ch in range(NCH - 1):
        direct(ch)

    loaded(l_sgu, sgu)
    loaded(l_sd)
    hidden = (jax.nn.silu(dot(ffn[...], sgu[0])) * dot(ffn[...], sgu[1])).astype(BF16)
    sh_s[...] = dot(hidden, sd[...]).astype(BF16)
    to_core(sh_s, sh_r, sh_r_sem).start()

    relay(0)
    direct(NCH - 1)
    relay(1)

    many = meta_r.at[pl.ds(0, NZ - 1)]
    remote(many, many, meta_sem.at[0], meta_sem.at[1], z_peer(1) * NQ + q, c).wait()
    meta = jnp.sum(meta_r[...], axis=0)
    code = meta[0:TOP, :].astype(jnp.int32)
    place = ((code % (2 * NQ)) // 2) * ROWS + (lane // SEQ) * 2 + code % 2
    place = jnp.where(code // (2 * NQ) == z, place, -1)
    row = lax.broadcasted_iota(jnp.int32, (NQ * ROWS, NZ * SEQ), 0)
    filled = jnp.zeros((NQ * ROWS, NZ * SEQ), F32)
    weight = jnp.zeros((NQ * ROWS, NZ * SEQ), F32)
    for k in range(TOP):
        hit = row == place[k : k + 1, :]
        filled = jnp.where(hit, 1.0, filled)
        weight = jnp.where(hit, meta[TOP + k : TOP + k + 1, :], weight)
    p_buf[...] = filled.astype(BF16)
    weight = weight.T
    high = weight.astype(BF16)
    whi[...] = high
    wlo[...] = (weight - high.astype(F32)).astype(BF16)

    def q_send(src, dst, rsem):
        for i in FAR:
            p = q_peer(i)
            remote(src.at[rows(p, ROWS)], dst.at[rows(q, ROWS)], chip_s, rsem, z * NQ + p, c).start()

    others = pl.ds(0, (NQ - 1) * ROWS)

    def picked(ch):
        arrived(g_buf[ch].at[pl.ds(0, 5 * SEQ)], za_r.at[ch])
        r_buf[ch][...] = dot(p_buf[...], g_buf[ch][...]).astype(BF16)
        q_send(r_buf[ch], x_buf[ch].at[c], xa_r.at[ch])
        x_buf[ch][c, rows(q, ROWS), :] = r_buf[ch][rows(q, ROWS), :]

    for ch in range(2, NCH):
        relay(ch)
        picked(ch - 2)
    picked(NCH - 2)
    picked(NCH - 1)

    loaded(l_egu, egu)
    gate = jnp.zeros((NQ * ROWS, HID), F32)
    up = jnp.zeros((NQ * ROWS, HID), F32)
    early = pl.ds(0, STARTS[-1])
    for ch in range(NCH):
        arrived(x_buf[ch].at[c, others], xa_r.at[ch])
        to_core(x_buf[ch].at[c], x_buf[ch].at[c], xf_r.at[ch // (NCH - 1)]).start()
        depth = pl.ds(pl.multiple_of(c * HALF + STARTS[ch], 128), WIDTHS[ch])
        gate += dot(x_buf[ch][c], egu[0, depth, :])
        up += dot(x_buf[ch][c], egu[1, depth, :])
    for ch in range(NCH):
        if ch == 0:
            arrived(wm.at[0, pl.ds(0, NQ * ROWS), early], xf_r.at[0])
        if ch == NCH - 1:
            arrived(x_buf[ch].at[1 - c], xf_r.at[1])
        depth = pl.ds(pl.multiple_of((1 - c) * HALF + STARTS[ch], 128), WIDTHS[ch])
        gate += dot(x_buf[ch][1 - c], egu[0, depth, :])
        up += dot(x_buf[ch][1 - c], egu[1, depth, :])
    hid_v[...] = (jax.nn.silu(gate) * up).astype(BF16)

    loaded(l_ed, ed)

    def down(core, ch):
        return dot(hid_v[...], ed[core, :, STARTS[ch] : STARTS[ch] + WIDTHS[ch]]).astype(BF16)

    def trade(ch):
        y_s[ch][...] = down(1 - c, ch)
        to_core(y_s[ch], y_r[ch], yx_r.at[ch]).start()

    def back(ch):
        own = down(c, ch).astype(F32)
        arrived(y_r[ch], yx_r.at[ch])
        o_buf[ch][...] = (own + y_r[ch][...].astype(F32)).astype(BF16)
        q_send(o_buf[ch], b_buf[ch], xb_r.at[ch])
        b_buf[ch][rows(q, ROWS), :] = o_buf[ch][rows(q, ROWS), :]

    trade(0)
    for ch in range(1, NCH):
        trade(ch)
        back(ch - 1)
    back(NCH - 1)

    def weighted(ch):
        arrived(b_buf[ch].at[others], xb_r.at[ch])
        t_buf[ch][...] = (dot(whi[...], b_buf[ch][...]) + dot(wlo[...], b_buf[ch][...])).astype(BF16)
        if ch == NCH - 1:
            for slot, i in enumerate((4, 3, -3, 2, -2, 1, -1)):
                to_z(t_buf[ch].at[rows(z_peer(i), SEQ)], v_buf[ch].at[slot], zb_r.at[1], i).start()
            return
        for way in range(2):
            sign = 1 - 2 * way
            if PLUS[ch] == way:
                to_z(t_buf[ch].at[rows(z_peer(4), SEQ)], rl_buf[ch].at[2], zb_two.at[ch], -2 * sign).start()
            to_z(t_buf[ch].at[rows(z_peer(-3 * sign), SEQ)], rl_buf[ch].at[way], zb_two.at[ch], -sign).start()
        for way in range(2):
            sign = 1 - 2 * way
            to_z(t_buf[ch].at[rows(z_peer(-sign), SEQ)], v_buf[ch].at[way], zb_r.at[0], -sign).start()

    def relayed(ch):
        arrived(rl_buf[ch], zb_two.at[ch])
        for way in range(2):
            sign = 1 - 2 * way
            total = t_buf[ch][rows(z_peer(-2 * sign), SEQ), :].astype(F32) + rl_buf[ch][way].astype(F32)
            if PLUS[ch] == way:
                total += rl_buf[ch][2].astype(F32)
            c_buf[ch][way] = total.astype(BF16)
            to_z(c_buf[ch].at[way], v_buf[ch].at[2 + way], zb_r.at[0], -2 * sign).start()

    weighted(0)
    for ch in range(1, NCH):
        weighted(ch)
        relayed(ch - 1)

    arrived(sh_r, sh_r_sem)

    def half(h):
        return pl.ds(pl.multiple_of(h * HALF, HALF), HALF)

    for ch in range(NCH):
        if ch == 0:
            arrived(wm.at[0, pl.ds(0, 4 * SEQ), early], zb_r.at[0])
        if ch == NCH - 1:
            arrived(v_buf[ch], zb_r.at[1])
        total = t_buf[ch][rows(z, SEQ), :].astype(F32)
        for s in range(7 if ch == NCH - 1 else 4):
            total += v_buf[ch][s].astype(F32)
        rt_buf[ch][c] = total.astype(BF16)
        to_core(rt_buf[ch].at[c], rt_buf[ch].at[c], rt_r_sem).start()

    def routed_and_shared(h):
        routed = jnp.concatenate([rt_buf[ch][h] for ch in range(NCH)], axis=1).astype(F32)
        return routed + (sh_s[:, half(h)].astype(F32) + sh_r[:, half(h)].astype(F32))

    def squares(value):
        return jnp.sum(value * value, axis=-1, keepdims=True)

    own = routed_and_shared(c)
    own_squares = squares(own)

    part = wm.at[:, pl.ds(0, (7 * SEQ + (NQ - 1) * ROWS))]
    to_z(part, part, zb_r.at[0], 1).wait_send()

    arrived(wm.at[0, pl.ds(0, SEQ)], rt_r_sem)
    other = routed_and_shared(1 - c)
    scale = lax.rsqrt((own_squares + squares(other)) / D + 1e-06)
    for h, value in ((c, own), (1 - c, other)):
        last = value * scale * gains[3, :, half(h)]
        out_v[:, half(h)] = (middle_v[:, half(h)].astype(F32) + last).astype(BF16)
    part = wm.at[:, pl.ds(0, (5 * SEQ + 2 * NQ * ROWS) // 2)]
    to_core(part, part, rt_r_sem).wait_send()


def store(*refs):
    n = len(refs) // 2
    copies = [pltpu.make_async_copy(refs[i], refs[n + i], refs[-1].at[i]) for i in range(n)]
    for copy in copies:
        copy.start()
    for copy in copies:
        copy.wait()


def on_device(
    tokens, lru_state, conv_window, gain_mix_in, gain_mix_out, gain_ffn_in, gain_ffn_out, w_branch, w_input,
    conv_taps, gate_a, gate_x, decay_rate, w_mix_out, routes, route_weight, expert_gate, expert_up, expert_down,
    shared_gate, shared_up, shared_down,
):
    hbm = pl.BlockSpec(memory_space=pltpu.HBM)

    def vmem(*shape, dtype=BF16):
        return pltpu.VMEM(shape, dtype)

    def chunks(*shape):
        return [vmem(*shape, width) for width in WIDTHS]

    def dma(*shape):
        return pltpu.SemaphoreType.DMA(shape)

    one = pltpu.SemaphoreType.DMA
    scratch = [
        vmem(SEQ, D), vmem(SEQ, LC, dtype=F32), vmem(3, SEQ, LC), vmem(4, LC), vmem(4, 1, D, dtype=F32),
        vmem(1, LC, dtype=F32), vmem(D, LC), vmem(D, LC), vmem(2, 4, 128, 128), vmem(2, LC, HALF),
        vmem(TOP, SEQ, dtype=jnp.int32), vmem(TOP, SEQ, dtype=F32),
        vmem(2, D, HID), vmem(2, HID, HALF), vmem(2, D, HID), vmem(HID, D),
        vmem(SEQ, D), vmem(SEQ, D),
        vmem(2, SEQ, HALF), vmem(2, SEQ, HALF), vmem(2 * TOP, NZ * SEQ, dtype=F32), vmem(NZ, 2 * TOP, NZ * SEQ, dtype=F32),
        vmem(SEQ, D), vmem(SEQ, D),
        chunks(NZ * SEQ), chunks(NQ * ROWS), chunks(2, NQ * ROWS),
        vmem(NQ * ROWS, NZ * SEQ), vmem(NZ * SEQ, NQ * ROWS), vmem(NZ * SEQ, NQ * ROWS), vmem(NQ * ROWS, HID),
        chunks(NQ * ROWS), chunks(NQ * ROWS), chunks(NQ * ROWS), chunks(NQ * ROWS),
        chunks(NZ * SEQ), chunks(3, SEQ), chunks(2, SEQ),
        [vmem(7 if ch == NCH - 1 else 4, SEQ, WIDTHS[ch]) for ch in range(NCH)], chunks(2, SEQ),
        dma(NLOAD), one, one, dma(2), dma(2), one, one,
        dma(NCH), dma(NCH), dma(NCH), dma(2), dma(NCH), dma(NCH), dma(NCH - 1), dma(2),
    ]
    vm = pl.BlockSpec(memory_space=pltpu.VMEM)
    results = pl.pallas_call(
        kernel,
        out_shape=(
            pltpu.VMEM((SEQ, D), BF16),
            pltpu.VMEM((SEQ, LC), F32),
            pltpu.VMEM((3, SEQ, LC), BF16),
        ),
        in_specs=[hbm] * 22,
        out_specs=(vm,) * 3,
        scratch_shapes=scratch,
        compiler_params=pltpu.CompilerParams(collective_id=0, has_side_effects=True, vmem_limit_bytes=60 * 2**20),
        name="layer",
    )(
        tokens, lru_state, conv_window.transpose(1, 0, 2), conv_taps, gain_mix_in[None], gain_mix_out[None],
        gain_ffn_in[None], gain_ffn_out[None], decay_rate[None], w_branch, w_input, gate_a, gate_x, w_mix_out,
        routes.T, route_weight.T, expert_gate, expert_up, expert_down[0], shared_gate, shared_up, shared_down,
    )
    layer_out, new_state, window = pl.pallas_call(
        store,
        out_shape=tuple(jax.ShapeDtypeStruct(r.shape, r.dtype) for r in results),
        in_specs=[vm] * 3,
        out_specs=(hbm,) * 3,
        scratch_shapes=[dma(3)],
        compiler_params=pltpu.CompilerParams(has_side_effects=True, vmem_limit_bytes=2**20),
        name="store",
    )(*results)
    return (layer_out, new_state, window.transpose(1, 0, 2))


def solution(mesh):
    placed = (
        P("ep", None),
        P("ep", "tp"),
        P("ep", None, "tp"),
        P(),
        P(),
        P(),
        P(),
        P(None, "tp"),
        P(None, "tp"),
        P(None, "tp"),
        P("tp", None, None),
        P("tp", None, None),
        P("tp"),
        P("tp", None),
        P("ep", None),
        P("ep", None),
        P("ep", None, "tp"),
        P("ep", None, "tp"),
        P("ep", "tp", None),
        P(None, "tp"),
        P(None, "tp"),
        P("tp", None),
    )
    return jax.shard_map(
        on_device,
        mesh=mesh,
        in_specs=placed,
        out_specs=(P("ep", None), P("ep", "tp"), P("ep", None, "tp")),
        check_vma=False,
    )
```

```python
import functools

import jax
import jax.numpy as jnp
from jax import lax
from jax.experimental import pallas as pl
from jax.experimental.pallas import tpu as pltpu
from jax.sharding import PartitionSpec as P

MESH = pl.DeviceIdType.MESH
F32 = jnp.float32
BF16 = jnp.bfloat16

NZ = 8
NQ = 16
SEQ = 32
TOP = 4
D = 2048
HALF = D // 2
WIDTHS = (256, 256, 256, 256)
NCH = len(WIDTHS)
STARTS = tuple(sum(WIDTHS[:i]) for i in range(NCH))
BACK_WIDTHS = (256, 512, 256)
NB = len(BACK_WIDTHS)
BACK_STARTS = tuple(sum(BACK_WIDTHS[:i]) for i in range(NB))
FAR = (10, 11, 9, 14, 6, 15, 5, 13, 7, 2, 8, 3, 1, 12, 4)
LC = 512
HID = 256
ROWS = NZ * 2
NLOAD = 24
PIECES = ((0, 512), (512, 512), (1024, 512), (1536, 512))


def scaled(value, gain):
    return value * lax.rsqrt(jnp.mean(value * value, axis=-1, keepdims=True) + 1e-06) * gain


def dot(a, b):
    return jnp.dot(a, b, preferred_element_type=F32)


def kernel(
    tok_h, lru_h, win_h, taps_h, gain0_h, gain1_h, gain2_h, gain3_h, decay_h, wb_h, wi_h, ga_h, gx_h, wm_h,
    routes_h, rweight_h, eg_h, eu_h, ed_h, sg_h, su_h, sd_h,
    out_v, state_v, window_v,
    tok, lru, win, taps, gains, decay, wb, wi, gax, wm, routes, rweight,
    egu, ed, sgu, sd,
    middle_v, ffn,
    mix_s, mix_r, meta_s, meta_r, sh_s, sh_r,
    g_buf, r_buf, x_buf, p_buf, whi, wlo, hid_v, y_s, y_r, o_buf, b_buf, t_buf, rl_buf, c_buf, v_buf, rt_buf,
    lsem, core_s, chip_s, meta_sem, mix_r_sem, sh_r_sem, rt_r_sem,
    za_two, za_r, xa_r, xf_r, yx_r, xb_r, zb_two, zb_r,
):
    me = lax.axis_index("ep")
    c = lax.axis_index("tp")
    z = me // NQ
    q = me % NQ
    y, x = q // 4, q % 4

    def z_peer(i):
        return lax.rem(z + (i + NZ), NZ)

    y_peer = [lax.rem(y + i, 4) * 4 for i in range(4)]
    x_peer = [lax.rem(x + i, 4) for i in range(4)]

    def q_peer(i):
        return y_peer[i // 4] + x_peer[i % 4]

    def rows(i, n):
        return pl.ds(pl.multiple_of(i * n, n), n)

    count = iter(range(NLOAD))

    def load(*pairs):
        k = next(count)
        copies = [pltpu.make_async_copy(src, dst, lsem.at[k]) for src, dst in pairs]
        for copy in copies:
            copy.start()
        return k, copies[0]

    def loaded(group, whole=None):
        k, copy = group
        if whole is not None:
            copy = pltpu.make_async_copy(whole, whole, lsem.at[k])
        copy.wait()

    l_tok = load((tok_h, tok))
    l_gain0 = load((gain0_h, gains.at[0]))
    l_wi = [load((wi_h.at[pl.ds(i, n)], wi.at[pl.ds(i, n)])) for i, n in PIECES]
    l_win = load((win_h, win))
    l_taps = load((taps_h, taps))
    l_gax = load((ga_h, gax.at[0]), (gx_h, gax.at[1]))
    l_decay = load((decay_h, decay))
    l_lru = load((lru_h, lru))
    l_wb = [load((wb_h.at[pl.ds(i, n)], wb.at[pl.ds(i, n)])) for i, n in PIECES]
    l_wm = [load((wm_h.at[:, pl.ds(i * HALF, HALF)], wm.at[i])) for i in range(2)]
    l_routes = load((routes_h, routes))
    l_rweight = load((rweight_h, rweight))
    l_gains = load((gain1_h, gains.at[1]), (gain2_h, gains.at[2]), (gain3_h, gains.at[3]))

    barrier = pltpu.get_barrier_semaphore()
    pl.semaphore_signal(barrier, inc=1, device_id=(me, 1 - c), device_id_type=MESH)

    def greet_z(i, carry):
        pl.semaphore_signal(barrier, inc=1, device_id=(z_peer(i) * NQ + q, c), device_id_type=MESH)
        return carry

    lax.fori_loop(1, NZ, greet_z, 0)
    for i in FAR:
        pl.semaphore_signal(barrier, inc=1, device_id=(z * NQ + q_peer(i), c), device_id_type=MESH)

    loaded(l_tok)
    loaded(l_gain0)
    normed = scaled(tok[...].astype(F32), gains[0]).astype(BF16)
    inflow = jnp.zeros((SEQ, LC), F32)
    for group, (i, n) in zip(l_wi, PIECES):
        loaded(group)
        inflow += dot(normed[:, i : i + n], wi[i : i + n, :])
    inflow = inflow.astype(BF16)
    loaded(l_win)
    loaded(l_taps)
    conv = inflow.astype(F32) * taps[3:4, :].astype(F32)
    for j in range(3):
        conv += win[j].astype(F32) * taps[j : j + 1, :].astype(F32)
        window_v[j] = win[j + 1] if j < 2 else inflow
    low = conv.astype(BF16)
    loaded(l_gax, gax)
    loaded(l_decay)
    loaded(l_lru)
    groups = LC // 128
    recur = [dot(low[:, g * 128 : (g + 1) * 128], gax[0, g]) for g in range(groups)]
    inputs = [dot(low[:, g * 128 : (g + 1) * 128], gax[1, g]) for g in range(groups)]
    recur_gate = jax.nn.sigmoid(jnp.concatenate(recur, axis=1))
    input_gate = jax.nn.sigmoid(jnp.concatenate(inputs, axis=1))
    fall = 8.0 * recur_gate * decay[...]
    t = jnp.tanh(fall)
    state = jnp.exp(-fall) * lru[...] + jnp.sqrt(2.0 * t / (1.0 + t)) * conv * input_gate
    state_v[...] = state
    branch = jnp.zeros((SEQ, LC), F32)
    for group, (i, n) in zip(l_wb, PIECES):
        loaded(group)
        branch += dot(normed[:, i : i + n], wb[i : i + n, :])
    gated = (state * jax.nn.gelu(branch)).astype(BF16)
    for i in range(2):
        loaded(l_wm[i])
        mix_s[i] = dot(gated, wm[i]).astype(BF16)

    l_sgu = load((sg_h, sgu.at[0]), (su_h, sgu.at[1]))
    l_sd = load((sd_h, sd))
    l_egu = load((eg_h.at[0], egu.at[0]), (eu_h.at[0], egu.at[1]))
    l_ed = load(*[(ed_h.at[:, pl.ds(i * HALF, HALF)], ed.at[i]) for i in range(2)])

    pl.semaphore_wait(barrier, 1 + (NZ - 1) + (NQ - 1))

    def remote(src, dst, ssem, rsem, e, t):
        return pltpu.make_async_remote_copy(
            src_ref=src, dst_ref=dst, send_sem=ssem, recv_sem=rsem, device_id=(e, t), device_id_type=MESH
        )

    def to_z(src, dst, rsem, i):
        return remote(src, dst, chip_s, rsem, z_peer(i) * NQ + q, c)

    def to_core(src, dst, rsem):
        return remote(src, dst, core_s, rsem, me, 1 - c)

    def arrived(ref, rsem):
        to_core(ref, ref, rsem).wait_recv()

    mix_copies = [to_core(mix_s.at[i], mix_r.at[i], mix_r_sem.at[i]) for i in range(2)]
    for copy in mix_copies:
        copy.start()

    with jax.named_scope("slots"):
        loaded(l_routes)
        loaded(l_rweight)
        lane = lax.broadcasted_iota(jnp.int32, (1, NZ * SEQ), 1)
        mine = (lane // SEQ) == z
        earlier = lax.broadcasted_iota(jnp.int32, (SEQ, NZ * SEQ), 0) < (lane % SEQ)
        diagonal = lax.broadcasted_iota(jnp.int32, (SEQ, SEQ), 0) == lax.broadcasted_iota(jnp.int32, (SEQ, SEQ), 1)
        narrow = routes[...].astype(F32)
        named = [
            jnp.sum(jnp.where(diagonal, narrow[k : k + 1, :], 0.0), axis=1, keepdims=True) for k in range(TOP)
        ]
        wide = jnp.concatenate([narrow] * NZ, axis=1)
        for k in range(TOP):
            expert = wide[k : k + 1, :]
            same = named[0] == expert
            for j in range(1, TOP):
                same = same | (named[j] == expert)
            rank = jnp.sum(jnp.where(same & earlier, 1.0, 0.0), axis=0, keepdims=True)
            meta_s[k : k + 1, :] = jnp.where(mine, 2.0 * expert + rank, 0.0)
        meta_s[TOP : 2 * TOP, :] = jnp.where(mine, jnp.concatenate([rweight[...]] * NZ, axis=1), 0.0)
        meta_r[pl.ds(z, 1)] = meta_s[...][None]

    def meta_send(i, carry):
        remote(meta_s, meta_r.at[z], meta_sem.at[0], meta_sem.at[1], z_peer(i) * NQ + q, c).start()
        return carry

    lax.fori_loop(1, NZ, meta_send, 0)

    loaded(l_gains, gains.at[pl.ds(1, 3)])
    mixed = []
    for i in range(2):
        mix_copies[i].wait_recv()
        mixed.append(mix_s[i].astype(F32) + mix_r[i].astype(F32))
    mixed = jnp.concatenate(mixed, axis=1)
    middle = (tok[...].astype(F32) + scaled(mixed, gains[1])).astype(BF16)
    middle_v[...] = middle
    ffn[...] = scaled(middle.astype(F32), gains[2]).astype(BF16)

    def z_copy(ch, source, i, rsem):
        block = g_buf[ch].at[rows(source, SEQ)]
        return to_z(block, block, rsem, i)

    def side(width, way):
        return pl.ds(way * width // 2, width // 2)

    def direct(ch):
        columns = pl.ds(pl.multiple_of(c * HALF + STARTS[ch], 128), WIDTHS[ch])
        g_buf[ch][rows(z, SEQ), :] = ffn[:, columns]
        z_copy(ch, z, 2, za_two.at[ch]).start()
        z_copy(ch, z, -2, za_two.at[ch]).start()
        z_copy(ch, z, 1, za_r.at[ch]).start()
        z_copy(ch, z, -1, za_r.at[ch]).start()

    def relay(ch):
        arrived(g_buf[ch].at[pl.ds(0, 2 * SEQ)], za_two.at[ch])
        for way in range(2):
            sign = 1 - 2 * way
            source = z_peer(-2 * sign)
            part = g_buf[ch].at[rows(source, SEQ), side(WIDTHS[ch], way)]
            to_z(part, part, za_r.at[ch], 2 * sign).start()
            z_copy(ch, source, sign, za_r.at[ch]).start()

    for ch in range(NCH - 1):
        direct(ch)

    loaded(l_sgu, sgu)
    loaded(l_sd)
    hidden = (jax.nn.silu(dot(ffn[...], sgu[0])) * dot(ffn[...], sgu[1])).astype(BF16)
    sh_s[...] = dot(hidden, sd[...]).astype(BF16)
    to_core(sh_s, sh_r, sh_r_sem).start()

    relay(0)
    direct(NCH - 1)
    relay(1)

    many = meta_r.at[pl.ds(0, NZ - 1)]
    remote(many, many, meta_sem.at[0], meta_sem.at[1], z_peer(1) * NQ + q, c).wait()
    meta = jnp.sum(meta_r[...], axis=0)
    code = meta[0:TOP, :].astype(jnp.int32)
    place = ((code % (2 * NQ)) // 2) * ROWS + (lane // SEQ) * 2 + code % 2
    place = jnp.where(code // (2 * NQ) == z, place, -1)
    row = lax.broadcasted_iota(jnp.int32, (NQ * ROWS, NZ * SEQ), 0)
    filled = jnp.zeros((NQ * ROWS, NZ * SEQ), F32)
    weight = jnp.zeros((NQ * ROWS, NZ * SEQ), F32)
    for k in range(TOP):
        hit = row == place[k : k + 1, :]
        filled = jnp.where(hit, 1.0, filled)
        weight = jnp.where(hit, meta[TOP + k : TOP + k + 1, :], weight)
    p_buf[...] = filled.astype(BF16)
    weight = weight.T
    high = weight.astype(BF16)
    whi[...] = high
    wlo[...] = (weight - high.astype(F32)).astype(BF16)

    def q_send(src, dst, rsem):
        for i in FAR:
            p = q_peer(i)
            remote(src.at[rows(p, ROWS)], dst.at[rows(q, ROWS)], chip_s, rsem, z * NQ + p, c).start()

    others = pl.ds(0, (NQ - 1) * ROWS)

    def picked(ch):
        arrived(g_buf[ch].at[pl.ds(0, 5 * SEQ)], za_r.at[ch])
        r_buf[ch][...] = dot(p_buf[...], g_buf[ch][...]).astype(BF16)
        q_send(r_buf[ch], x_buf[ch].at[c], xa_r.at[ch])
        x_buf[ch][c, rows(q, ROWS), :] = r_buf[ch][rows(q, ROWS), :]

    for ch in range(2, NCH):
        relay(ch)
        picked(ch - 2)
    picked(NCH - 2)
    picked(NCH - 1)

    loaded(l_egu, egu)
    gate = jnp.zeros((NQ * ROWS, HID), F32)
    up = jnp.zeros((NQ * ROWS, HID), F32)
    early = pl.ds(0, STARTS[-1])
    for ch in range(NCH):
        arrived(x_buf[ch].at[c, others], xa_r.at[ch])
        to_core(x_buf[ch].at[c], x_buf[ch].at[c], xf_r.at[ch // (NCH - 1)]).start()
        depth = pl.ds(pl.multiple_of(c * HALF + STARTS[ch], 128), WIDTHS[ch])
        gate += dot(x_buf[ch][c], egu[0, depth, :])
        up += dot(x_buf[ch][c], egu[1, depth, :])
    for ch in range(NCH):
        if ch == 0:
            arrived(wm.at[0, pl.ds(0, NQ * ROWS), early], xf_r.at[0])
        if ch == NCH - 1:
            arrived(x_buf[ch].at[1 - c], xf_r.at[1])
        depth = pl.ds(pl.multiple_of((1 - c) * HALF + STARTS[ch], 128), WIDTHS[ch])
        gate += dot(x_buf[ch][1 - c], egu[0, depth, :])
        up += dot(x_buf[ch][1 - c], egu[1, depth, :])
    hid_v[...] = (jax.nn.silu(gate) * up).astype(BF16)

    loaded(l_ed, ed)

    def down(core, ch):
        return dot(hid_v[...], ed[core, :, BACK_STARTS[ch] : BACK_STARTS[ch] + BACK_WIDTHS[ch]]).astype(BF16)

    def trade(ch):
        y_s[ch][...] = down(1 - c, ch)
        to_core(y_s[ch], y_r[ch], yx_r.at[ch]).start()

    def back(ch):
        own = down(c, ch).astype(F32)
        arrived(y_r[ch], yx_r.at[ch])
        o_buf[ch][...] = (own + y_r[ch][...].astype(F32)).astype(BF16)
        q_send(o_buf[ch], b_buf[ch], xb_r.at[ch])
        b_buf[ch][rows(q, ROWS), :] = o_buf[ch][rows(q, ROWS), :]

    trade(0)
    for ch in range(1, NB):
        trade(ch)
        back(ch - 1)
    back(NB - 1)

    def weighted(ch):
        arrived(b_buf[ch].at[others], xb_r.at[ch])
        t_buf[ch][...] = (dot(whi[...], b_buf[ch][...]) + dot(wlo[...], b_buf[ch][...])).astype(BF16)
        if ch == NB - 1:
            for slot, i in enumerate((4, 3, -3, 2, -2, 1, -1)):
                to_z(t_buf[ch].at[rows(z_peer(i), SEQ)], v_buf[ch].at[slot], zb_r.at[1], i).start()
            return
        for way in range(2):
            sign = 1 - 2 * way
            part = side(BACK_WIDTHS[ch], way)
            to_z(t_buf[ch].at[rows(z_peer(4), SEQ), part], rl_buf[ch].at[2, :, part], zb_two.at[ch], -2 * sign).start()
            to_z(t_buf[ch].at[rows(z_peer(-3 * sign), SEQ)], rl_buf[ch].at[way], zb_two.at[ch], -sign).start()
        for way in range(2):
            sign = 1 - 2 * way
            to_z(t_buf[ch].at[rows(z_peer(-sign), SEQ)], v_buf[ch].at[way], zb_r.at[0], -sign).start()

    def relayed(ch):
        arrived(rl_buf[ch], zb_two.at[ch])
        for way in range(2):
            sign = 1 - 2 * way
            total = t_buf[ch][rows(z_peer(-2 * sign), SEQ), :].astype(F32) + rl_buf[ch][way].astype(F32)
            mid = BACK_WIDTHS[ch] // 2
            far = rl_buf[ch][2, :, way * mid : (way + 1) * mid].astype(F32)
            sides = [total[:, :mid], total[:, mid:]]
            sides[way] += far
            c_buf[ch][way] = jnp.concatenate(sides, axis=1).astype(BF16)
            to_z(c_buf[ch].at[way], v_buf[ch].at[2 + way], zb_r.at[0], -2 * sign).start()

    weighted(0)
    for ch in range(1, NB):
        weighted(ch)
        relayed(ch - 1)

    arrived(sh_r, sh_r_sem)

    def half(h):
        return pl.ds(pl.multiple_of(h * HALF, HALF), HALF)

    for ch in range(NB):
        if ch == 0:
            arrived(wm.at[0, pl.ds(0, 4 * SEQ), pl.ds(0, BACK_STARTS[-1])], zb_r.at[0])
        if ch == NB - 1:
            arrived(v_buf[ch], zb_r.at[1])
        total = t_buf[ch][rows(z, SEQ), :].astype(F32)
        for s in range(7 if ch == NB - 1 else 4):
            total += v_buf[ch][s].astype(F32)
        rt_buf[ch][c] = total.astype(BF16)
        to_core(rt_buf[ch].at[c], rt_buf[ch].at[c], rt_r_sem).start()

    def routed_and_shared(h):
        routed = jnp.concatenate([rt_buf[ch][h] for ch in range(NB)], axis=1).astype(F32)
        return routed + (sh_s[:, half(h)].astype(F32) + sh_r[:, half(h)].astype(F32))

    def squares(value):
        return jnp.sum(value * value, axis=-1, keepdims=True)

    own = routed_and_shared(c)
    own_squares = squares(own)

    part = wm.at[:, pl.ds(0, (7 * SEQ + (NQ - 1) * ROWS))]
    to_z(part, part, zb_r.at[0], 1).wait_send()

    arrived(wm.at[0, pl.ds(0, SEQ)], rt_r_sem)
    other = routed_and_shared(1 - c)
    scale = lax.rsqrt((own_squares + squares(other)) / D + 1e-06)
    for h, value in ((c, own), (1 - c, other)):
        last = value * scale * gains[3, :, half(h)]
        out_v[:, half(h)] = (middle_v[:, half(h)].astype(F32) + last).astype(BF16)
    part = wm.at[:, pl.ds(0, (5 * SEQ + 2 * NQ * ROWS) // 2)]
    to_core(part, part, rt_r_sem).wait_send()


def store(*refs):
    n = len(refs) // 2
    copies = [pltpu.make_async_copy(refs[i], refs[n + i], refs[-1].at[i]) for i in range(n)]
    for copy in copies:
        copy.start()
    for copy in copies:
        copy.wait()


def on_device(
    tokens, lru_state, conv_window, gain_mix_in, gain_mix_out, gain_ffn_in, gain_ffn_out, w_branch, w_input,
    conv_taps, gate_a, gate_x, decay_rate, w_mix_out, routes, route_weight, expert_gate, expert_up, expert_down,
    shared_gate, shared_up, shared_down,
):
    hbm = pl.BlockSpec(memory_space=pltpu.HBM)

    def vmem(*shape, dtype=BF16):
        return pltpu.VMEM(shape, dtype)

    def chunks(*shape, widths=WIDTHS):
        return [vmem(*shape, width) for width in widths]

    backs = functools.partial(chunks, widths=BACK_WIDTHS)

    def dma(*shape):
        return pltpu.SemaphoreType.DMA(shape)

    one = pltpu.SemaphoreType.DMA
    scratch = [
        vmem(SEQ, D), vmem(SEQ, LC, dtype=F32), vmem(3, SEQ, LC), vmem(4, LC), vmem(4, 1, D, dtype=F32),
        vmem(1, LC, dtype=F32), vmem(D, LC), vmem(D, LC), vmem(2, 4, 128, 128), vmem(2, LC, HALF),
        vmem(TOP, SEQ, dtype=jnp.int32), vmem(TOP, SEQ, dtype=F32),
        vmem(2, D, HID), vmem(2, HID, HALF), vmem(2, D, HID), vmem(HID, D),
        vmem(SEQ, D), vmem(SEQ, D),
        vmem(2, SEQ, HALF), vmem(2, SEQ, HALF), vmem(2 * TOP, NZ * SEQ, dtype=F32), vmem(NZ, 2 * TOP, NZ * SEQ, dtype=F32),
        vmem(SEQ, D), vmem(SEQ, D),
        chunks(NZ * SEQ), chunks(NQ * ROWS), chunks(2, NQ * ROWS),
        vmem(NQ * ROWS, NZ * SEQ), vmem(NZ * SEQ, NQ * ROWS), vmem(NZ * SEQ, NQ * ROWS), vmem(NQ * ROWS, HID),
        backs(NQ * ROWS), backs(NQ * ROWS), backs(NQ * ROWS), backs(NQ * ROWS),
        backs(NZ * SEQ), backs(3, SEQ), backs(2, SEQ),
        [vmem(7 if ch == NB - 1 else 4, SEQ, BACK_WIDTHS[ch]) for ch in range(NB)], backs(2, SEQ),
        dma(NLOAD), one, one, dma(2), dma(2), one, one,
        dma(NCH), dma(NCH), dma(NCH), dma(2), dma(NB), dma(NB), dma(NB - 1), dma(2),
    ]
    vm = pl.BlockSpec(memory_space=pltpu.VMEM)
    results = pl.pallas_call(
        kernel,
        out_shape=(
            pltpu.VMEM((SEQ, D), BF16),
            pltpu.VMEM((SEQ, LC), F32),
            pltpu.VMEM((3, SEQ, LC), BF16),
        ),
        in_specs=[hbm] * 22,
        out_specs=(vm,) * 3,
        scratch_shapes=scratch,
        compiler_params=pltpu.CompilerParams(collective_id=0, has_side_effects=True, vmem_limit_bytes=60 * 2**20),
        name="layer",
    )(
        tokens, lru_state, conv_window.transpose(1, 0, 2), conv_taps, gain_mix_in[None], gain_mix_out[None],
        gain_ffn_in[None], gain_ffn_out[None], decay_rate[None], w_branch, w_input, gate_a, gate_x, w_mix_out,
        routes.T, route_weight.T, expert_gate, expert_up, expert_down[0], shared_gate, shared_up, shared_down,
    )
    layer_out, new_state, window = pl.pallas_call(
        store,
        out_shape=tuple(jax.ShapeDtypeStruct(r.shape, r.dtype) for r in results),
        in_specs=[vm] * 3,
        out_specs=(hbm,) * 3,
        scratch_shapes=[dma(3)],
        compiler_params=pltpu.CompilerParams(has_side_effects=True, vmem_limit_bytes=2**20),
        name="store",
    )(*results)
    return (layer_out, new_state, window.transpose(1, 0, 2))


def solution(mesh):
    placed = (
        P("ep", None),
        P("ep", "tp"),
        P("ep", None, "tp"),
        P(),
        P(),
        P(),
        P(),
        P(None, "tp"),
        P(None, "tp"),
        P(None, "tp"),
        P("tp", None, None),
        P("tp", None, None),
        P("tp"),
        P("tp", None),
        P("ep", None),
        P("ep", None),
        P("ep", None, "tp"),
        P("ep", None, "tp"),
        P("ep", "tp", None),
        P(None, "tp"),
        P(None, "tp"),
        P("tp", None),
    )
    return jax.shard_map(
        on_device,
        mesh=mesh,
        in_specs=placed,
        out_specs=(P("ep", None), P("ep", "tp"), P("ep", None, "tp")),
        check_vma=False,
    )
```
